512 devices in a mesh: ep: 128 (over z, y, core), tp: 4 (over x).
Axes of the slice: x: 4, y: 8, z: 8, core: 2. Of those that a mesh axis runs over, the one named last changes fastest.
Arguments:
- tokens: bfloat16 [2048, 1024], P(('ep', 'tp')), may hold values from -6 to 6
- lengths: int32 [2048], P('ep'), may hold values from 256 to 1024
- key_cache: bfloat16 [2048, 1024, 128], P(('ep', 'tp')), may hold values from -1500 to 1500
- value_cache: bfloat16 [2048, 1024, 128], P(('ep', 'tp')), may hold values from -6 to 6
- query_weight: bfloat16 [1024, 512], P(None, 'tp'), may hold values from -0.1875 to 0.1875
- key_weight: bfloat16 [1024, 128], replicated, may hold values from -0.1875 to 0.1875
- value_weight: bfloat16 [1024, 128], replicated, may hold values from -0.1875 to 0.1875
- lambdas: float32 [4], replicated, may hold values from 0.3 to 0.8
- head_gain: float32 [128], replicated, may hold values from 0.1 to 1.9
- output_weight: bfloat16 [512, 1024], P(None, 'tp'), may hold values from -0.25 to 0.25
- norm1_gain: float32 [1024], replicated, may hold values from 0.1 to 1.9
- routes: int32 [2048, 6], P('ep'), may hold values from 0 to 127, all different within a row; in each aligned block of 16 rows (0 to 15, 16 to 31, ...) at most 2 rows name the same one
- route_logits: float32 [2048, 6], P('ep'), may hold values from -9 to 410
- gate_weight: bfloat16 [128, 1024, 1024], P('ep', None, 'tp'), may hold values from -0.5 to 0.5
- up_weight: bfloat16 [128, 1024, 1024], P('ep', None, 'tp'), may hold values from -0.5 to 0.5
- down_weight: bfloat16 [128, 1024, 1024], P('ep', 'tp'), may hold values from -0.09375 to 0.09375
- norm2_gain: float32 [1024], replicated, may hold values from 0.1 to 1.9
Outputs:
- mixed: bfloat16 [2048, 1024], P('ep', 'tp')
The draws below stay inside these ranges and needn't reach their ends.
Inputs may be any that keep to these rules, and one draw needn't show every extreme that they name: `routes`: in the 16 rows of each aligned block (the rows held by one index of ep) no expert is named by more than 2 rows, a bound that some block reaches; the experts of a row differ.
All inputs are finite; a program needn't handle non-finite values.
Results may differ from the reference program's by a relative error of at most 0.014.
Values may be sent and summed in bfloat16 or wider, within the bound.
A program may use at most 64 MiB of HBM per device.

```python
import math
import jax
import jax.numpy as jnp
import numpy as np
from jax import lax

D = 1024
HEADS = 4
DH = 64
VH = 128
FF = 1024
TOPK = 6
CACHE = 1024
TOK_GRP = 16
BATCH = 2048
EXPERTS = 128
CAP = 2
N_EP = 128
N_TP = 4


def draw_key_cache(key, part):
    base = jnp.clip(jax.random.normal(key, (BATCH, CACHE, 2 * DH), jnp.float32) * 1.75, -9.0, 9.0)
    return base.astype(jnp.bfloat16)


def draw_route_logits(key, part):
    base = jnp.clip(jax.random.normal(key, (BATCH, TOPK), jnp.float32) * 1.5, -9.0, 9.0)
    return base


def touch_ends(values, key, smallest, top_value):
    index_at = [jax.random.randint(jax.random.fold_in(key, axis), (), 0, length) for axis, length in enumerate(values.shape)]
    longest = values.shape.index(max(values.shape))
    neighbour = index_at[:longest] + [(index_at[longest] + 1) % values.shape[longest]] + index_at[longest + 1:]
    return values.at[tuple(index_at)].set(smallest).at[tuple(neighbour)].set(top_value)


def block_levels(key, extent, cuts, least, largest):
    level = 1.0
    for axis_at, parts in cuts:
        heights = jax.random.uniform(jax.random.fold_in(jax.random.fold_in(key, 6), axis_at), (parts,), jnp.float32, least / len(cuts), largest / len(cuts))
        level = level * jnp.repeat(jnp.exp(heights), extent[axis_at] // parts).reshape((-1,) + (1,) * (len(extent) - 1 - axis_at))
    return level


def deal_out(own_key, own, number, rows, amount, top, bound, lean):
    sequence = jax.random.permutation(own_key, amount)
    heavy_load, ordinary = load_shares(amount, rows * top, bound, lean, True), load_shares(amount, rows * top, bound, lean, False)
    places = jnp.arange(amount)

    def named(sizes, rotation):
        used = int((sizes > 0).sum())
        fixed = max(1, used // 4)
        moved = fixed + (places - fixed + rotation * (used - fixed)) % max(1, amount - fixed)
        return jnp.zeros((amount,), jnp.int32).at[sequence[jnp.where(places < fixed, places, moved)]].set(jnp.asarray(sizes, jnp.int32))

    sizes = jnp.where(number % 4 == 0, named(heavy_load, number // 4), named(ordinary, number - number // 4 - 1))
    mixed = jax.random.permutation(jax.random.fold_in(own, 3), amount)
    source_of, receiver = mixed[0:amount // 2 * 2:2], mixed[1:amount // 2 * 2:2]
    room = jnp.minimum(sizes[source_of] - 1, bound - sizes[receiver]) // 2
    room = jnp.where((source_of == sequence[0]) | (receiver == sequence[0]) | (sizes[receiver] == 0), 0, jnp.maximum(room, 0))
    moved = jax.random.randint(jax.random.fold_in(own, 4), (amount // 2,), 0, 1 << 20) % (room + 1)
    sizes = sizes.at[source_of].add(-moved).at[receiver].add(moved)
    members = jnp.searchsorted(jnp.cumsum(sizes), jnp.arange(rows * top), side="right").astype(jnp.int32)
    grid = members.reshape(top, rows).T
    grid = grid[jax.random.permutation(jax.random.fold_in(own, 1), rows)]
    rotation = jax.random.randint(jax.random.fold_in(own, 2), (rows, 1), 0, top)
    return jnp.take_along_axis(grid, (jnp.arange(top)[None, :] + rotation) % top, axis=1)


def load_shares(number_of, total, reach, skew, full):
    weights = [(1 << 20) // math.isqrt(grade ** skew) + 1 for grade in range(1, number_of + 1)]
    largest = reach if full else min(reach, max(-(-total // number_of), total * weights[0] // sum(weights)))
    least = 1 if total - largest >= number_of - 1 else 0
    given, rest = [largest] + [least] * (number_of - 1), total - largest - least * (number_of - 1)
    while rest > 0:
        candidates = [i for i in range(1, number_of) if given[i] < largest] or [i for i in range(1, number_of) if given[i] < reach]
        whole, budget = sum([weights[i] for i in candidates]), rest
        for i in candidates:
            more = min(reach - given[i], max(1, budget * weights[i] // whole), rest)
            given[i] = given[i] + more
            rest = rest - more
    return np.array(given)


def gaussian(key, shape, scale, most, cuts=(), kind=jnp.bfloat16):
    entries = jax.random.normal(key, shape, jnp.float32) * scale
    if len(cuts) > 0:
        entries = block_levels(key, shape, cuts, -0.22, 0.18) * entries
    return jnp.clip(entries, min=-most, max=most).astype(kind)


def setup_inputs(seed: int = 0) -> dict:
    key_list = jax.random.split(jax.random.key(seed), 18)
    tokens = gaussian(key_list[0], (BATCH, D), 1.0, 6.0, ((0, 512),))
    lengths = touch_ends(jax.random.randint(key_list[1], (BATCH,), CACHE // 4, CACHE + 1), jax.random.fold_in(key_list[1], 1), CACHE // 4, CACHE).astype(jnp.int32)
    key_cache = draw_key_cache(jax.random.fold_in(key_list[17], 71), 0)
    value_cache = gaussian(key_list[3], (BATCH, CACHE, VH), 1.0, 6.0, ((0, 512),))
    query_weight = gaussian(key_list[4], (D, 2 * DH * HEADS), D ** -0.5, 0.1875, ((1, 4),))
    key_weight = gaussian(key_list[5], (D, 2 * DH), D ** -0.5, 0.1875)
    value_weight = gaussian(key_list[6], (D, VH), D ** -0.5, 0.1875)
    lambdas = jnp.clip(jax.random.uniform(key_list[7], (HEADS,), jnp.float32, 0.3, 0.8), 0.3, 0.8)
    head_gain = jnp.clip(1.0 + 0.18 * jax.random.normal(key_list[8], (VH,), jnp.float32), 0.1, 1.9)
    output_weight = gaussian(key_list[9], (HEADS * VH, D), (HEADS * VH) ** -0.5, 0.25, ((1, 4),))
    norm1_gain = jnp.clip(1.0 + 0.18 * jax.random.normal(key_list[10], (D,), jnp.float32), 0.1, 1.9)
    routes_keys = jax.random.split(jax.random.fold_in(key_list[11], 1), BATCH // TOK_GRP)
    routes_turns = jax.random.permutation(jax.random.fold_in(key_list[11], 3), BATCH // TOK_GRP)
    routes = jax.vmap(lambda own, number: deal_out(jax.random.fold_in(key_list[11], 2), own, number, TOK_GRP, EXPERTS, TOPK, CAP, 2))(routes_keys, routes_turns).reshape((BATCH, TOPK))
    route_logits = draw_route_logits(jax.random.fold_in(key_list[17], 71), 0)
    gate_weight = gaussian(key_list[13], (EXPERTS, D, FF), (D // 9) ** -0.5, 0.5, ((0, 128), (2, 4)))
    up_weight = gaussian(key_list[14], (EXPERTS, D, FF), (D // 9) ** -0.5, 0.5, ((0, 128), (2, 4)))
    down_weight = gaussian(key_list[15], (EXPERTS, FF, D), (4 * FF) ** -0.5, 0.09375, ((0, 128), (1, 4)))
    norm2_gain = jnp.clip(1.0 + 0.18 * jax.random.normal(key_list[16], (D,), jnp.float32), 0.1, 1.9)
    return {"tokens": tokens, "lengths": lengths, "key_cache": key_cache, "value_cache": value_cache, "query_weight": query_weight, "key_weight": key_weight, "value_weight": value_weight, "lambdas": lambdas, "head_gain": head_gain, "output_weight": output_weight, "norm1_gain": norm1_gain, "routes": routes, "route_logits": route_logits, "gate_weight": gate_weight, "up_weight": up_weight, "down_weight": down_weight, "norm2_gain": norm2_gain}


ALPHA = 1.4142135623730951
EPS = 1e-05
THETA = 500000.0
LIMIT = 7.0
SLOPE = 1.702

def rotate(values, positions):
    half = values.shape[-1] // 2
    freqs = THETA ** (-jnp.arange(half, dtype=jnp.float32) / half)
    angles = positions.astype(jnp.float32)[:, None] * freqs[None, :]
    shape = (angles.shape[0],) + (1,) * (values.ndim - 2) + (half,)
    cosine = jnp.cos(angles).reshape(shape)
    sine = jnp.sin(angles).reshape(shape)
    first = values[..., :half]
    second = values[..., half:]
    return jnp.concatenate([first * cosine - second * sine, second * cosine + first * sine], axis=-1)

def norm_rows(summed, gain):
    mean = lax.optimization_barrier(jnp.mean(summed, axis=-1, keepdims=True))
    center = summed - mean
    spread = lax.optimization_barrier(jnp.mean(center * center, axis=-1, keepdims=True))
    return center * lax.rsqrt(spread + EPS) * gain

def choose_slots(routes_block, experts, capacity):
    flat = routes_block.reshape(-1).astype(jnp.int32)
    onehot = (flat[:, None] == jnp.arange(experts, dtype=jnp.int32)[None, :]).astype(jnp.int32)
    before = jnp.cumsum(onehot, axis=0) - onehot
    slot = lax.optimization_barrier(jnp.sum(before * onehot, axis=1))
    target = flat * capacity + slot
    return target[:, None] == jnp.arange(experts * capacity, dtype=jnp.int32)[None, :]

def attend_block(query, new_key, new_value, keys, values, lengths, lambdas, head_gain):
    f32 = jnp.float32
    count, length = (keys.shape[0], keys.shape[1])
    keys = keys.reshape(count, length, 2, -1)
    scale = keys.shape[-1] ** (-0.5)
    past = jnp.einsum('bhmd,bjmd->bhmj', query.astype(f32), keys.astype(f32)) * scale
    live = jnp.arange(length, dtype=jnp.int32)[None, :] < lengths[:, None]
    past = jnp.where(live[:, None, None, :], past, -jnp.inf)
    selfs = jnp.einsum('bhmd,bmd->bhm', query.astype(f32), new_key.astype(f32)) * scale
    top = jnp.maximum(lax.optimization_barrier(jnp.max(past, axis=-1)), selfs)
    past_exp = jnp.exp(past - top[..., None])
    self_exp = jnp.exp(selfs - top)
    total = lax.optimization_barrier(jnp.sum(past_exp, axis=-1)) + self_exp
    past_prob = past_exp / total[..., None]
    self_prob = self_exp / total
    mixing = lambdas[None, :]
    past_weight = (past_prob[:, :, 0] - mixing[..., None] * past_prob[:, :, 1]).astype(jnp.bfloat16)
    self_weight = (self_prob[:, :, 0] - mixing * self_prob[:, :, 1]).astype(jnp.bfloat16)
    head_out = jnp.einsum('bhj,bje->bhe', past_weight.astype(f32), values.astype(f32))
    head_out = head_out + self_weight.astype(f32)[..., None] * new_value.astype(f32)[:, None, :]
    normed = head_out * lax.rsqrt(lax.optimization_barrier(jnp.mean(head_out * head_out, axis=-1, keepdims=True)) + EPS) * head_gain
    return normed.astype(jnp.bfloat16).reshape(count, -1)

def reference(tokens, lengths, key_cache, value_cache, query_weight, key_weight, value_weight, lambdas, head_gain, output_weight, norm1_gain, routes, route_logits, gate_weight, up_weight, down_weight, norm2_gain):
    f32 = jnp.float32
    bf16 = jnp.bfloat16
    rows = tokens.shape[0]
    query = jnp.dot(tokens, query_weight, preferred_element_type=f32).reshape(rows, HEADS, 2, DH)
    query = rotate(query, lengths).astype(bf16)
    new_key = jnp.dot(tokens, key_weight, preferred_element_type=f32).reshape(rows, 2, DH)
    new_key = rotate(new_key, lengths).astype(bf16)
    new_value = jnp.dot(tokens, value_weight, preferred_element_type=f32).astype(bf16)

    def one_group(pieces):
        return attend_block(*pieces, lambdas, head_gain)
    grouped = tuple((a.reshape((N_EP, TOK_GRP) + a.shape[1:]) for a in (query, new_key, new_value, key_cache, value_cache, lengths)))
    attended = lax.map(one_group, grouped).reshape(rows, HEADS * VH)
    summed = ALPHA * tokens.astype(f32) + jnp.dot(attended, output_weight, preferred_element_type=f32)
    settled = norm_rows(summed, norm1_gain).astype(bf16)
    route_weight = jax.nn.softmax(route_logits, axis=-1)
    routes_grouped = routes.reshape(N_EP, TOK_GRP, TOPK)

    def dispatch(pieces):
        rows_block, routes_block = pieces
        chosen = choose_slots(routes_block, EXPERTS, CAP)
        placing = lax.optimization_barrier(jnp.sum(chosen.reshape(TOK_GRP, TOPK, -1).astype(f32), axis=1)).astype(bf16)
        sent = jnp.dot(placing.T, rows_block, preferred_element_type=f32)
        return sent.astype(bf16)
    sends = lax.map(dispatch, (settled.reshape(N_EP, TOK_GRP, D), routes_grouped))
    sends = jnp.moveaxis(sends.reshape(N_EP, EXPERTS, CAP, D), 1, 0)
    block = FF // N_TP

    def run_expert(pieces):
        rows_e, gate_e, up_e, down_e = pieces
        gate_h = jnp.einsum('scd,df->scf', rows_e.astype(f32), gate_e.astype(f32))
        up_h = jnp.einsum('scd,df->scf', rows_e.astype(f32), up_e.astype(f32))
        clipped = jnp.minimum(gate_h, LIMIT)
        linear = jnp.clip(up_h, -LIMIT, LIMIT)
        act = (clipped * jax.nn.sigmoid(SLOPE * clipped) * (linear + 1.0)).astype(bf16)
        total = jnp.zeros(rows_e.shape, f32)
        for index in range(N_TP):
            piece = jnp.einsum('scf,fd->scd', act[..., index * block:(index + 1) * block].astype(f32), down_e[index * block:(index + 1) * block].astype(f32))
            rounded = lax.optimization_barrier(piece.astype(bf16))
            total = total + rounded.astype(f32)
        return total.astype(bf16)
    answers = lax.map(run_expert, (sends, gate_weight, up_weight, down_weight))
    answers = jnp.moveaxis(answers, 1, 0).reshape(N_EP, EXPERTS * CAP, D)

    def combine(pieces):
        answers_block, routes_block = pieces
        chosen = choose_slots(routes_block, EXPERTS, CAP)
        picked = jnp.dot(chosen.astype(bf16), answers_block, preferred_element_type=f32)
        return picked.reshape(TOK_GRP, TOPK, D)
    picked = lax.map(combine, (answers, routes_grouped)).reshape(rows, TOPK, D)
    routed = lax.optimization_barrier(jnp.sum(picked * route_weight[:, :, None], axis=1))
    return norm_rows(ALPHA * settled.astype(f32) + routed, norm2_gain).astype(bf16)
```

```python
import functools

import jax
import jax.numpy as jnp
from jax import lax
from jax.experimental import pallas as pl
from jax.experimental.pallas import tpu as pltpu
from jax.sharding import PartitionSpec as P

ALPHA = 1.4142135623730951
EPS = 1e-05
THETA = 500000.0
LIMIT = 7.0
SLOPE = 1.702
LANES = 128
MESH = pl.DeviceIdType.MESH
BF16 = jnp.bfloat16
F32 = jnp.float32


def log2(n):
    return n.bit_length() - 1


def iota(shape, dim):
    return lax.broadcasted_iota(jnp.int32, shape, dim)


def ones_where(mask):
    return jnp.where(mask, 1.0, 0.0)


def dot(a, b):
    return jnp.dot(a, b, preferred_element_type=F32)


def zigzag(i, n):
    step = (i + 1) // 2
    return lax.rem(n // 2 + (1 - 2 * ((i + 1) % 2)) * step + n, n)


class Sizes:
    def __init__(self, nz, nyc, tp, own, blocks, heads, length, topk, cap):
        self.nz, self.nyc, self.tp, self.own = nz, nyc, tp, own
        self.blocks, self.heads, self.length = blocks, heads, length
        self.topk, self.cap = topk, cap
        self.group = own * tp
        self.rows = nz * nyc * cap
        self.zrows = nyc * cap
        self.yrows = nz * cap


class Exchange:
    def __init__(self, sizes, along_z, ep, out, into, send, recv):
        self.sizes, self.along_z, self.ep = sizes, along_z, ep
        self.out, self.into, self.send, self.recv = out, into, send, recv
        self.count = sizes.nz if along_z else sizes.nyc

    def peer(self, i):
        s = self.sizes
        z, yc = self.ep // s.nyc, self.ep % s.nyc
        if self.along_z:
            other = lax.rem(z + zigzag(i, s.nz), s.nz)
            return other, other * s.nyc + yc
        ny = s.nyc // 2
        y, c = yc // 2, yc % 2
        other = lax.rem(y + zigzag(i // 2, ny), ny) * 2 + lax.rem(c + 1 - i % 2, 2)
        return other, z * s.nyc + other

    def me(self):
        return self.ep // self.sizes.nyc if self.along_z else self.ep % self.sizes.nyc

    def copy(self, i):
        other, device = self.peer(i)
        return pltpu.make_async_remote_copy(
            src_ref=self.out.at[other],
            dst_ref=self.into.at[self.me()],
            send_sem=self.send.at[i],
            recv_sem=self.recv.at[i],
            device_id={"ep": device},
            device_id_type=MESH,
        )

    def loop(self, action):
        def step(i, carry):
            action(i)
            return carry

        lax.fori_loop(0, self.count - 1, step, 0)

    def start(self):
        self.loop(lambda i: self.copy(i).start())
        mine = self.me()
        self.into[mine] = self.out[mine]

    def wait_recv(self):
        self.loop(lambda i: self.copy(i).wait_recv())

    def wait_send(self):
        self.loop(lambda i: self.copy(i).wait_send())


def kernel(
    s,
    tok_ref,
    len_ref,
    cos_ref,
    sin_ref,
    routes_ref,
    routes_t_ref,
    logits_ref,
    lam_ref,
    hgain_ref,
    gain1_ref,
    gain2_ref,
    wq_hbm,
    wk_hbm,
    wv_hbm,
    wo_hbm,
    kc_hbm,
    vc_hbm,
    gate_hbm,
    up_hbm,
    down_hbm,
    out_ref,
    wq,
    wk,
    wv,
    wo,
    kc,
    vc,
    gate,
    up,
    down,
    tokbuf,
    xs,
    qbuf,
    nk_s,
    nv_s,
    attbuf,
    stats1,
    stats2,
    pzy,
    pyz,
    pla,
    plb,
    ca,
    cb,
    dz1o,
    dz1i,
    dy1o,
    dy1i,
    dy2o,
    dz2o,
    dz2i,
    xb,
    gacc,
    uacc,
    r2o,
    r2i,
    rdo,
    rdi,
    rpo,
    rpi,
    ey1o,
    ey1i,
    ez2o,
    ez2i,
    ez1o,
    ez1i,
    ey2o,
    ey2i,
    load_sem,
    tp_send,
    tp_recv,
    x_send,
    x_recv,
    z_send,
    z_recv,
    y_send,
    y_recv,
):
    ep = lax.axis_index("ep")
    t = lax.axis_index("tp")
    tp, own, group, heads = s.tp, s.own, s.group, s.heads
    rows, cap = s.rows, s.cap
    part = 2 * LANES
    nxt = lax.rem(t + 1, tp)
    far = lax.rem(t + 2, tp)
    prv = lax.rem(t + 3, tp)

    pairs = [
        (wq_hbm, wq),
        (wk_hbm, wk),
        (wv_hbm, wv),
        (kc_hbm, kc),
        (vc_hbm, vc),
        (wo_hbm, wo),
        (gate_hbm, gate),
        (up_hbm, up),
        (down_hbm, down),
    ]
    loads = [pltpu.make_async_copy(a, b, load_sem.at[i]) for i, (a, b) in enumerate(pairs)]

    barrier = pltpu.get_barrier_semaphore()
    probe_z = Exchange(s, True, ep, None, None, None, None)
    probe_y = Exchange(s, False, ep, None, None, None, None)

    def greet(device):
        pl.semaphore_signal(barrier, inc=1, device_id=device, device_id_type=MESH)

    probe_z.loop(lambda i: greet({"ep": probe_z.peer(i)[1]}))
    probe_y.loop(lambda i: greet({"ep": probe_y.peer(i)[1]}))
    for d in range(1, tp):
        greet({"tp": lax.rem(t + d, tp)})
    for load in loads:
        load.start()

    lc, lz = log2(cap), log2(s.nz)

    def slots(r, z_major):
        slot = r & (cap - 1)
        if z_major:
            return r >> lc, slot
        z = (r >> lc) & (s.nz - 1)
        return z * s.nyc + (r >> (lc + lz)), slot

    r0, c0 = iota((rows, rows), 0), iota((rows, rows), 1)
    lyc = log2(s.nyc)
    z_of, yc_of = (r0 >> lc) & (s.nz - 1), r0 >> (lc + lz)
    pzy[...] = ones_where(c0 == (z_of * s.nyc + yc_of) * cap + (r0 & (cap - 1))).astype(BF16)
    yc_of, z_of = (r0 >> lc) & (s.nyc - 1), r0 >> (lc + lyc)
    pyz[...] = ones_where(c0 == (yc_of * s.nz + z_of) * cap + (r0 & (cap - 1))).astype(BF16)

    logits = logits_ref[...]
    raised = jnp.exp(logits - jnp.max(logits, axis=-1, keepdims=True))
    route_weight = raised / jnp.sum(raised, axis=-1, keepdims=True)
    upper = ones_where(iota((group, group), 0) < iota((group, group), 1)).astype(BF16)
    lower = ones_where(iota((group, group), 1) < iota((group, group), 0)).astype(BF16)
    for z_major, pl_ref, c_ref in ((True, pla, ca), (False, plb, cb)):
        expert, slot = slots(iota((rows, group), 0), z_major)
        named = jnp.zeros((rows, group), F32)
        for k in range(s.topk):
            named += ones_where(routes_t_ref[k : k + 1, :] == expert)
        before = dot(named.astype(BF16), upper)
        pl_ref[...] = jnp.where(before == slot.astype(F32), named, 0.0).astype(BF16)
        expert, slot = slots(iota((group, rows), 1), z_major)
        named = jnp.zeros((group, rows), F32)
        weighed = jnp.zeros((group, rows), F32)
        for k in range(s.topk):
            hit = routes_ref[:, k : k + 1] == expert
            named += ones_where(hit)
            weighed += jnp.where(hit, route_weight[:, k : k + 1], 0.0)
        before = dot(lower, named.astype(BF16))
        weighed = jnp.where(before == slot.astype(F32), weighed, 0.0)
        for i in range(3):
            piece = weighed.astype(BF16)
            c_ref[i * group : (i + 1) * group, :] = piece
            weighed = weighed - piece.astype(F32)

    def tp_copies(phase, src, buf):
        return [
            pltpu.make_async_remote_copy(
                src_ref=src,
                dst_ref=buf.at[t],
                send_sem=tp_send.at[phase, d - 1],
                recv_sem=tp_recv.at[phase, d - 1],
                device_id={"tp": lax.rem(t + d, tp)},
                device_id_type=MESH,
            )
            for d in (2, 1, 3)
        ]

    sent = []

    def gather(phase, src, buf):
        copies = tp_copies(phase, src, buf)
        for copy in copies:
            copy.start()
        sent.extend(copies)
        return copies

    def arrived(copies):
        for copy in copies:
            copy.wait_recv()

    tokbuf[t] = tok_ref[...]
    pl.semaphore_wait(barrier, s.nz - 1 + s.nyc - 1 + tp - 1)

    copies = gather(0, tok_ref, tokbuf)
    nrow = tp * s.blocks * own
    r0, c0 = iota((nrow, nrow), 0), iota((nrow, nrow), 1)
    lo, lt, lb = log2(own), log2(tp), log2(s.blocks)
    origin = (((r0 >> lo) & (tp - 1)) << (lb + lo)) + ((r0 >> (lo + lt)) << lo) + (r0 & (own - 1))
    order = ones_where(c0 == origin).astype(BF16)
    loads[0].wait()
    arrived(copies)
    x = dot(order, tokbuf[...].reshape(nrow, LANES)).astype(BF16)
    xs[...] = x.reshape(s.blocks, group, LANES)
    x = jnp.concatenate([xs[i] for i in range(s.blocks)], axis=-1)

    cosine, sine = cos_ref[...], sin_ref[...]
    lane = iota((group, LANES), 1)

    def rotate(v):
        swapped = jnp.where((lane & 32) == 0, pltpu.roll(v, 96, 1), pltpu.roll(v, 32, 1))
        return (v * cosine + swapped * sine).astype(BF16)

    qbuf[t] = rotate(dot(x, wq[...]))
    copies = gather(1, qbuf.at[t], qbuf)
    loads[1].wait()
    loads[2].wait()
    nk_s[...] = rotate(dot(x, wk[...])).astype(F32)
    nv_s[...] = dot(x, wv[...]).astype(BF16).astype(F32)

    lh = log2(heads)
    nq = own * 2 * heads
    r0, c0 = iota((nq, heads * group), 0), iota((nq, heads * group), 1)
    source = ((r0 & (heads - 1)) * group) + t * own + (r0 >> (lh + 1))
    order = ones_where(c0 == source).astype(BF16)
    loads[3].wait()
    loads[4].wait()
    arrived(copies)
    q = dot(order, qbuf[...].reshape(heads * group, LANES))
    q = jnp.where((iota((nq, LANES), 1) >> 6) == ((iota((nq, LANES), 0) >> lh) & 1), q, 0.0)
    position = iota((2 * heads, s.length), 1)
    head = iota((2 * heads, 1), 0) & (heads - 1)
    lam = jnp.zeros((2 * heads, 1), F32)
    for h in range(heads):
        lam = jnp.where(head == h, lam_ref[h], lam)
    outs = []
    for b in range(own):
        qb = q[b * 2 * heads : (b + 1) * 2 * heads, :]
        score = lax.dot_general(
            qb.astype(BF16), kc[b], (((1,), (1,)), ((), ())), preferred_element_type=F32
        )
        score = jnp.where(position < len_ref[t * own + b], score * 0.125, -jnp.inf)
        own_score = jnp.sum(qb * nk_s[pl.ds(t * own + b, 1), :], axis=-1, keepdims=True) * 0.125
        top = jnp.maximum(jnp.max(score, axis=-1, keepdims=True), own_score)
        e = jnp.exp(score - top)
        e_own = jnp.exp(own_score - top)
        total = jnp.sum(e, axis=-1, keepdims=True) + e_own
        prob = e / total
        prob_own = jnp.broadcast_to(e_own / total, (2 * heads, LANES))
        weight = (prob - lam * pltpu.roll(prob, heads, 0)).astype(BF16)
        weight_own = (prob_own - lam * pltpu.roll(prob_own, heads, 0)).astype(BF16).astype(F32)
        ho = dot(weight, vc[b]) + weight_own * nv_s[pl.ds(t * own + b, 1), :]
        scale = lax.rsqrt(jnp.mean(ho * ho, axis=-1, keepdims=True) + EPS)
        outs.append(ho * scale * hgain_ref[...])
    attbuf[t] = jnp.concatenate(outs, axis=0).astype(BF16)

    copies = gather(2, attbuf.at[t], attbuf)
    r0, c0 = iota((heads * group, tp * nq), 0), iota((heads * group, tp * nq), 1)
    lg = log2(group)
    token = r0 & (group - 1)
    source = (token >> lo) * nq + (token & (own - 1)) * (2 * heads) + (r0 >> lg)
    order = ones_where(c0 == source).astype(BF16)
    loads[5].wait()
    columns = jnp.concatenate([xs[2 * t], xs[2 * t + 1]], axis=-1).astype(F32)
    arrived(copies)
    att = dot(order, attbuf[...].reshape(tp * nq, LANES)).astype(BF16)
    att = jnp.concatenate([att[h * group : (h + 1) * group, :] for h in range(heads)], axis=-1)
    summed = ALPHA * columns + dot(att, wo[...])

    def normed(v, phase, stats, gain):
        mean = jnp.mean(v, axis=-1, keepdims=True)
        center = v - mean
        square = jnp.sum(center * center, axis=-1, keepdims=True)
        stats[t] = jnp.where(lane == 0, mean, jnp.where(lane == 1, square, 0.0))
        arrived(gather(phase, stats.at[t], stats))
        means = [stats[i][:, 0:1] for i in range(tp)]
        squares = [stats[i][:, 1:2] for i in range(tp)]
        mean = sum(means) / tp
        spread = (sum(squares) + part * sum((m - mean) ** 2 for m in means)) / (tp * part)
        return ((v - mean) * lax.rsqrt(spread + EPS) * gain[pl.ds(t, 1), :]).astype(BF16)

    settled = normed(summed, 3, stats1, gain1_ref)

    nz, nyc, zrows, yrows = s.nz, s.nyc, s.zrows, s.yrows
    xmine = xb.at[t, 0]
    dza = Exchange(s, True, ep, dz1o, dz1i, z_send.at[0], z_recv.at[0])
    dyb = Exchange(s, False, ep, dy1o, dy1i, y_send.at[0], y_recv.at[0])
    dya = Exchange(s, False, ep, dy2o, xmine, y_send.at[1], y_recv.at[1])
    dzb = Exchange(s, True, ep, dz2o, dz2i, z_send.at[1], z_recv.at[1])
    dz1o[...] = dot(pla[...], settled[:, :LANES]).astype(BF16).reshape(nz, zrows, LANES)
    dza.start()
    dy1o[...] = dot(plb[...], settled[:, LANES:]).astype(BF16).reshape(nyc, yrows, LANES)
    dyb.start()
    dza.wait_recv()
    moved = dot(pzy[...], dz1i[...].reshape(rows, LANES)).astype(BF16)
    dy2o[...] = moved.reshape(nyc, yrows, LANES)
    dya.start()
    dyb.wait_recv()
    moved = dot(pyz[...], dy1i[...].reshape(rows, LANES)).astype(BF16)
    dz2o[...] = moved.reshape(nz, zrows, LANES)
    dzb.start()

    def x_copy(i, src, dst, to):
        copy = pltpu.make_async_remote_copy(
            src_ref=src,
            dst_ref=dst,
            send_sem=x_send.at[i],
            recv_sem=x_recv.at[i],
            device_id={"tp": to},
            device_id_type=MESH,
        )
        sent.append(copy)
        return copy

    a_next = x_copy(0, xb.at[t, 0], xb.at[t, 0], nxt)
    b_next = x_copy(1, xb.at[t, 1], xb.at[t, 1], nxt)
    a_prev = x_copy(2, xb.at[t, 0], xb.at[t, 0], prv)
    b_prev = x_copy(3, xb.at[t, 1], xb.at[t, 1], prv)
    a_pass = x_copy(4, xb.at[prv, 0], xb.at[prv, 0], nxt)
    b_pass = x_copy(5, xb.at[nxt, 1], xb.at[nxt, 1], prv)
    dya.wait_recv()
    a_next.start()
    dzb.wait_recv()
    moved = dot(pzy[...], dz2i[...].reshape(rows, LANES)).astype(BF16)
    xb[t, 1] = moved.reshape(nyc, yrows, LANES)
    b_prev.start()
    b_next.start()
    a_prev.start()
    loads[6].wait()
    loads[7].wait()

    def hidden(i):
        x = jnp.concatenate([xb[i, 0].reshape(rows, LANES), xb[i, 1].reshape(rows, LANES)], axis=-1)
        at = pl.ds(pl.multiple_of(i * part, part), part)
        return dot(x, gate[at, :]), dot(x, up[at, :])

    g, u = hidden(t)
    gacc[...] = g
    uacc[...] = u
    a_next.wait_recv()
    a_pass.start()
    b_prev.wait_recv()
    b_pass.start()
    b_next.wait_recv()
    g, u = hidden(prv)
    gacc[...] += g
    uacc[...] += u
    a_prev.wait_recv()
    g, u = hidden(nxt)
    gacc[...] += g
    uacc[...] += u
    loads[8].wait()
    a_pass.wait_recv()
    b_pass.wait_recv()
    g, u = hidden(far)
    g = jnp.minimum(gacc[...] + g, LIMIT)
    u = jnp.clip(uacc[...] + u, -LIMIT, LIMIT)
    act = (g / (1.0 + jnp.exp(-SLOPE * g)) * (u + 1.0)).astype(BF16)

    def terms(i):
        return dot(act, down[:, pl.ds(pl.multiple_of(i * part, part), part)])

    a_far = x_copy(6, r2o.at[0], r2i.at[0], nxt)
    b_far = x_copy(7, r2o.at[1], r2i.at[1], prv)
    b_near = x_copy(8, rdo.at[0], rdi.at[0], nxt)
    a_near = x_copy(9, rdo.at[1], rdi.at[1], prv)
    a_pair = x_copy(10, rpo.at[0], rpi.at[0], nxt)
    b_pair = x_copy(11, rpo.at[1], rpi.at[1], prv)
    v = terms(far)
    r2o[0] = v[:, :LANES].astype(BF16)
    a_far.start()
    r2o[1] = v[:, LANES:].astype(BF16)
    b_far.start()
    vn = terms(nxt)
    rdo[0] = vn[:, LANES:].astype(BF16)
    b_near.start()
    vp = terms(prv)
    rdo[1] = vp[:, :LANES].astype(BF16)
    a_near.start()
    a_far.wait_recv()
    rpo[0] = (vn[:, :LANES] + r2i[0].astype(F32)).astype(BF16)
    a_pair.start()
    b_far.wait_recv()
    rpo[1] = (vp[:, LANES:] + r2i[1].astype(F32)).astype(BF16)
    b_pair.start()
    v = terms(t)
    eya = Exchange(s, False, ep, ey1o, ey1i, y_send.at[2], y_recv.at[2])
    ezb = Exchange(s, True, ep, ez1o, ez1i, z_send.at[2], z_recv.at[2])
    eza = Exchange(s, True, ep, ez2o, ez2i, z_send.at[3], z_recv.at[3])
    eyb = Exchange(s, False, ep, ey2o, ey2i, y_send.at[3], y_recv.at[3])
    a_near.wait_recv()
    a_pair.wait_recv()
    answer = v[:, :LANES] + rpi[0].astype(F32) + rdi[1].astype(F32)
    ey1o[...] = answer.astype(BF16).reshape(nyc, yrows, LANES)
    eya.start()
    b_near.wait_recv()
    b_pair.wait_recv()
    answer = v[:, LANES:] + rpi[1].astype(F32) + rdi[0].astype(F32)
    moved = dot(pyz[...], answer.astype(BF16)).astype(BF16)
    ez1o[...] = moved.reshape(nz, zrows, LANES)
    ezb.start()
    eya.wait_recv()
    moved = dot(pyz[...], ey1i[...].reshape(rows, LANES)).astype(BF16)
    ez2o[...] = moved.reshape(nz, zrows, LANES)
    eza.start()
    ezb.wait_recv()
    moved = dot(pzy[...], ez1i[...].reshape(rows, LANES)).astype(BF16)
    ey2o[...] = moved.reshape(nyc, yrows, LANES)
    eyb.start()

    def combined(c_ref, back):
        three = dot(c_ref[...], back[...].reshape(rows, LANES))
        return three[:group] + three[group : 2 * group] + three[2 * group :]

    eza.wait_recv()
    routed_a = combined(ca, ez2i)
    eyb.wait_recv()
    routed_b = combined(cb, ey2i)
    final = ALPHA * settled.astype(F32) + jnp.concatenate([routed_a, routed_b], axis=-1)
    out_ref[...] = normed(final, 4, stats2, gain2_ref)

    for copy in sent:
        copy.wait_send()
    for exchange in (dza, dyb, dya, dzb, eya, ezb, eza, eyb):
        exchange.wait_send()


def layer(
    nz,
    cap,
    tokens,
    lengths,
    key_cache,
    value_cache,
    query_weight,
    key_weight,
    value_weight,
    lambdas,
    head_gain,
    output_weight,
    norm1_gain,
    routes,
    route_logits,
    gate_weight,
    up_weight,
    down_weight,
    norm2_gain,
):
    tp = lax.axis_size("tp")
    own, width = tokens.shape
    blocks = width // LANES
    group = own * tp
    heads = lambdas.shape[0]
    length = key_cache.shape[1]
    s = Sizes(
        nz, lax.axis_size("ep") // nz, tp, own, blocks, heads, length, routes.shape[1], cap
    )
    half = key_weight.shape[1] // 4
    freqs = THETA ** (-jnp.arange(half, dtype=F32) / half)
    angles = lengths.astype(F32)[:, None] * freqs[None, :]
    cosine, sine = jnp.cos(angles), jnp.sin(angles)
    cosine = jnp.concatenate([cosine] * 4, axis=1)
    sine = jnp.concatenate([-sine, sine, -sine, sine], axis=1)
    rows, part = s.rows, width // tp
    tok = tokens.reshape(own, blocks, LANES).transpose(1, 0, 2).reshape(blocks * own, LANES)
    vmem = pl.BlockSpec(memory_space=pltpu.VMEM)
    smem = pl.BlockSpec(memory_space=pltpu.SMEM)
    hbm = pl.BlockSpec(memory_space=pl.ANY)

    def b(*shape):
        return pltpu.VMEM(shape, BF16)

    def f(*shape):
        return pltpu.VMEM(shape, F32)

    by_z = (nz, s.zrows, LANES)
    by_y = (s.nyc, s.yrows, LANES)
    sem = pltpu.SemaphoreType.DMA
    large = [query_weight, key_weight, value_weight, output_weight, key_cache, value_cache]
    large += [gate_weight[0], up_weight[0], down_weight[0]]
    landing = [large[i] for i in (0, 1, 2, 3, 4, 5, 6, 7, 8)]
    return pl.pallas_call(
        functools.partial(kernel, s),
        out_shape=jax.ShapeDtypeStruct((group, part), BF16),
        in_specs=[vmem, smem] + [vmem] * 5 + [smem] + [vmem] * 3 + [hbm] * 9,
        out_specs=vmem,
        scratch_shapes=[pltpu.VMEM(a.shape, a.dtype) for a in landing]
        + [
            b(tp, blocks * own, LANES),
            b(blocks, group, LANES),
            b(tp, group, LANES),
            f(group, LANES),
            f(group, LANES),
            b(tp, own * 2 * heads, LANES),
            f(tp, group, LANES),
            f(tp, group, LANES),
            b(rows, rows),
            b(rows, rows),
            b(rows, group),
            b(rows, group),
            b(3 * group, rows),
            b(3 * group, rows),
            b(*by_z),
            b(*by_z),
            b(*by_y),
            b(*by_y),
            b(*by_y),
            b(*by_z),
            b(*by_z),
            b(tp, 2, *by_y),
            f(rows, down_weight.shape[1]),
            f(rows, down_weight.shape[1]),
        ]
        + [b(2, rows, LANES)] * 6
        + [b(*by_y), b(*by_y), b(*by_z), b(*by_z)]
        + [b(*by_z), b(*by_z), b(*by_y), b(*by_y)]
        + [
            sem((9,)),
            sem((5, tp - 1)),
            sem((5, tp - 1)),
            sem((12,)),
            sem((12,)),
            sem((4, nz - 1)),
            sem((4, nz - 1)),
            sem((4, s.nyc - 1)),
            sem((4, s.nyc - 1)),
        ],
        compiler_params=pltpu.CompilerParams(collective_id=0, has_side_effects=True),
    )(
        tok,
        lengths,
        cosine,
        sine,
        routes,
        routes.T,
        route_logits,
        lambdas,
        head_gain.reshape(1, -1),
        norm1_gain.reshape(tp, part),
        norm2_gain.reshape(tp, part),
        *large,
    )


def solution(mesh, nz=8, cap=2):
    in_specs = (
        P(("ep", "tp"), None),
        P("ep"),
        P(("ep", "tp"), None, None),
        P(("ep", "tp"), None, None),
        P(None, "tp"),
        P(),
        P(),
        P(),
        P(),
        P(None, "tp"),
        P(),
        P("ep", None),
        P("ep", None),
        P("ep", None, "tp"),
        P("ep", None, "tp"),
        P("ep", "tp", None),
        P(),
    )
    return jax.shard_map(
        functools.partial(layer, nz, cap),
        mesh=mesh,
        in_specs=in_specs,
        out_specs=P("ep", "tp"),
        check_vma=False,
    )
```

```python
import functools

import jax
import jax.numpy as jnp
import numpy as np
from jax import lax
from jax.experimental import pallas as pl
from jax.experimental.pallas import tpu as pltpu
from jax.sharding import PartitionSpec as P

ALPHA = 1.4142135623730951
EPS = 1e-05
THETA = 500000.0
LIMIT = 7.0
SLOPE = 1.702
LANES = 128
SMALL = ("lens", "freqs", "routes", "logits", "lams", "hgain", "gain1", "gain2")
NAMES = SMALL + ("wq", "wk", "wv", "kc", "vc", "wo", "gate", "up", "down")
MESH = pl.DeviceIdType.MESH
BF16 = jnp.bfloat16
F32 = jnp.float32


def log2(n):
    return n.bit_length() - 1


def iota(shape, dim):
    return lax.broadcasted_iota(jnp.int32, shape, dim)


def ones_where(mask):
    return jnp.where(mask, 1.0, 0.0)


def dot(a, b):
    return jnp.dot(a, b, preferred_element_type=F32)


def zigzag(i, n):
    step = (i + 1) // 2
    return lax.rem(n // 2 + (1 - 2 * ((i + 1) % 2)) * step + n, n)


class Sizes:
    def __init__(self, nz, nyc, tp, own, blocks, heads, length, topk, cap):
        self.nz, self.nyc, self.tp, self.own = nz, nyc, tp, own
        self.blocks, self.heads, self.length = blocks, heads, length
        self.topk, self.cap = topk, cap
        self.group = own * tp
        self.experts = nz * nyc
        self.rows = nz * nyc * cap


class Exchange:
    def __init__(self, sizes, ep, out, into, send, recv):
        self.sizes, self.ep = sizes, ep
        self.out, self.into, self.send, self.recv = out, into, send, recv

    def peer(self, i):
        s = self.sizes
        z, y, c = self.ep // s.nyc, self.ep % s.nyc // 2, self.ep % 2
        j = i % s.nyc
        z = lax.rem(z + zigzag(i // s.nyc, s.nz), s.nz)
        y = lax.rem(y + zigzag(j // 2, s.nyc // 2), s.nyc // 2)
        return z * s.nyc + y * 2 + lax.rem(c + 1 - j % 2, 2)

    def start(self):
        def step(i, carry):
            other = self.peer(i)
            pltpu.make_async_remote_copy(
                src_ref=self.out.at[:, other],
                dst_ref=self.into.at[:, self.ep],
                send_sem=self.send,
                recv_sem=self.recv,
                device_id={"ep": other},
                device_id_type=MESH,
            ).start()
            return carry

        lax.fori_loop(0, self.sizes.experts - 1, step, 0)
        for half in range(2):
            self.into[half, self.ep] = self.out[half, self.ep]

    def total(self):
        every = pl.ds(0, self.sizes.experts - 1)
        return pltpu.make_async_remote_copy(
            src_ref=self.out.at[:, every],
            dst_ref=self.into.at[:, every],
            send_sem=self.send,
            recv_sem=self.recv,
            device_id={"ep": lax.rem(self.ep + 1, self.sizes.experts)},
            device_id_type=MESH,
        )

    def wait_recv(self):
        self.total().wait_recv()

    def wait_send(self):
        self.total().wait_send()


def rotation(angle):
    turns = jnp.floor(angle * 0.6366197723675814 + 0.5)
    r = angle - turns * 1.5703125
    r = r - turns * 4.837512969970703125e-4
    r = r - turns * 7.54978995489188216e-8
    q = r * r
    sine = r + r * q * (-1.6666654611e-1 + q * (8.3321608736e-3 - q * 1.9515295891e-4))
    cosine = 4.166664568298827e-2 + q * (-1.388731625493765e-3 + q * 2.443315711809948e-5)
    cosine = 1.0 - 0.5 * q + q * q * cosine
    quarter = turns.astype(jnp.int32)
    odd = (quarter & 1) == 1
    c = jnp.where(odd, sine, cosine)
    n = jnp.where(odd, cosine, sine)
    c = jnp.where(((quarter + 1) & 2) == 2, -c, c)
    n = jnp.where((quarter & 2) == 2, -n, n)
    return c, n


def kernel(
    s,
    *refs,
):
    count = len(NAMES)
    tok_hbm, inputs, out_ref = refs[0], refs[1 : count + 1], refs[count + 1]
    landing, refs = refs[count + 2 : 2 * count + 2], refs[2 * count + 2 :]
    (lens, freqs, routes_t, logits_t, lams, hgain, gain1, gain2) = landing[:8]
    (wq, wk, wv, kc, vc, wo, gate, up, down) = landing[8:]
    (tokbuf, xs, qbuf, nk_s, nv_s, len_s, attbuf, stats1, stats2, place, pick) = refs[:11]
    (dout, xb, gacc, uacc, r2o, r2i, rdo, rdi, rpo, rpi, eout, einto) = refs[11:23]
    (load_sem, tp_send, tp_recv, x_send, x_recv, ep_send, ep_recv, here) = refs[23:]
    ep = lax.axis_index("ep")
    t = lax.axis_index("tp")
    tp, own, group, heads = s.tp, s.own, s.group, s.heads
    rows, cap = s.rows, s.cap
    part = 2 * LANES
    nxt = lax.rem(t + 1, tp)
    far = lax.rem(t + 2, tp)
    prv = lax.rem(t + 3, tp)

    barrier = pltpu.get_barrier_semaphore()
    nz, ny = s.nz, s.nyc // 2
    z, y, c = ep // s.nyc, ep % s.nyc // 2, ep % 2

    def at_z(d):
        return {"ep": lax.rem(z + d + nz, nz) * s.nyc + ep % s.nyc}

    def at_y(d):
        return {"ep": z * s.nyc + lax.rem(y + d + ny, ny) * 2 + c}

    across = {"ep": ep + 1 - 2 * c}

    def pair(at, d, n):
        return [at(e) for e in sorted({d % n, -d % n} - {0})]

    near = pair(at_z, 1, nz) + pair(at_y, 1, ny) + [across]
    near += [{"tp": lax.rem(t + d, tp)} for d in range(1, tp)]
    for device in near:
        pl.semaphore_signal(barrier, inc=1, device_id=device, device_id_type=MESH)

    rounds = [
        pair(at_z, 1, nz),
        pair(at_z, 2, nz),
        pair(at_y, 1, ny),
        pair(at_y, 2, ny),
        pair(at_y, 4, ny),
        [across],
    ]

    def tell(i):
        for device in rounds[i]:
            pl.semaphore_signal(here.at[i], inc=1, device_id=device, device_id_type=MESH)

    def heard(i):
        if rounds[i]:
            pl.semaphore_wait(here.at[i], len(rounds[i]))

    tok_load = pltpu.make_async_copy(tok_hbm, tokbuf.at[t], load_sem.at[len(inputs)])
    tok_load.start()
    loads = {}
    for i, name in enumerate(NAMES):
        loads[name] = pltpu.make_async_copy(inputs[i], landing[i], load_sem.at[i])
        loads[name].start()

    for name in NAMES[:8]:
        loads[name].wait()
    lc = log2(cap)
    logits = logits_t[...]
    raised = jnp.exp(logits - jnp.max(logits, axis=0, keepdims=True))
    left = raised / jnp.sum(raised, axis=0, keepdims=True)
    named = routes_t[...].astype(F32)
    r0, c0 = iota((group, group), 0), iota((group, group), 1)
    upper = ones_where(r0 < c0).astype(BF16)
    lower = ones_where(c0 < r0).astype(BF16)
    same = ones_where(c0 == r0).astype(BF16)

    def upright(v):
        return lax.dot_general(
            same, v.astype(BF16), (((1,), (1,)), ((), ())), preferred_element_type=F32
        )

    routes = upright(named)
    pieces = []
    for i in range(3):
        pieces.append(left.astype(BF16))
        left = left - pieces[-1].astype(F32)
    route_weight = sum(upright(piece) for piece in pieces)
    row = iota((rows, group), 0)
    hits = jnp.zeros((rows, group), F32)
    for k in range(s.topk):
        hits += ones_where(named[k : k + 1, :] == (row >> lc).astype(F32))
    before = dot(hits.astype(BF16), upper)
    place[...] = jnp.where(before == (row & (cap - 1)).astype(F32), hits, 0.0).astype(BF16)
    row = iota((group, rows), 1)
    hits = jnp.zeros((group, rows), F32)
    weighed = jnp.zeros((group, rows), F32)
    for k in range(s.topk):
        hit = routes[:, k : k + 1] == (row >> lc).astype(F32)
        hits += ones_where(hit)
        weighed += jnp.where(hit, route_weight[:, k : k + 1], 0.0)
    before = dot(lower, hits.astype(BF16))
    weighed = jnp.where(before == (row & (cap - 1)).astype(F32), weighed, 0.0)
    for i in range(3):
        piece = weighed.astype(BF16)
        pick[i * group : (i + 1) * group, :] = piece
        weighed = weighed - piece.astype(F32)

    lane = iota((group, LANES), 1)
    lengths = jnp.where(c0 == r0, lens[...].astype(F32), 0.0)
    lengths = jnp.broadcast_to(jnp.sum(lengths, axis=-1, keepdims=True), (group, LANES))
    len_s[...] = lengths
    cosine, sine = rotation(lengths * freqs[...])
    sine = jnp.where((lane & 32) == 0, -sine, sine)
    r0, c0 = iota((2 * heads, heads), 0), iota((2 * heads, heads), 1)
    lam = jnp.where((r0 & (heads - 1)) == c0, lams[...], 0.0)
    lam = jnp.sum(lam, axis=-1, keepdims=True)

    def tp_copies(phase, src, buf):
        return [
            pltpu.make_async_remote_copy(
                src_ref=src,
                dst_ref=buf.at[t],
                send_sem=tp_send.at[phase, d - 1],
                recv_sem=tp_recv.at[phase, d - 1],
                device_id={"tp": lax.rem(t + d, tp)},
                device_id_type=MESH,
            )
            for d in (2, 1, 3)
        ]

    sent = []

    def gather(phase, src, buf):
        copies = tp_copies(phase, src, buf)
        for copy in copies:
            copy.start()
        sent.extend(copies)
        return copies

    def arrived(copies):
        for copy in copies:
            copy.wait_recv()

    tok_load.wait()
    pl.semaphore_wait(barrier, len(near))

    copies = gather(0, tokbuf.at[t], tokbuf)
    tell(0)
    nrow = tp * s.blocks * own
    r0, c0 = iota((nrow, nrow), 0), iota((nrow, nrow), 1)
    lo, lt, lb = log2(own), log2(tp), log2(s.blocks)
    origin = (((r0 >> lo) & (tp - 1)) << (lb + lo)) + ((r0 >> (lo + lt)) << lo) + (r0 & (own - 1))
    order = ones_where(c0 == origin).astype(BF16)
    loads["wq"].wait()
    arrived(copies)
    x = dot(order, tokbuf[...].reshape(nrow, LANES)).astype(BF16)
    xs[...] = x.reshape(s.blocks, group, LANES)
    x = jnp.concatenate([xs[i] for i in range(s.blocks)], axis=-1)

    def rotate(v):
        swapped = jnp.where((lane & 32) == 0, pltpu.roll(v, 96, 1), pltpu.roll(v, 32, 1))
        return (v * cosine + swapped * sine).astype(BF16)

    qbuf[t] = rotate(dot(x, wq[...]))
    copies = gather(1, qbuf.at[t], qbuf)
    heard(0)
    tell(1)
    loads["wk"].wait()
    loads["wv"].wait()
    nk_s[...] = rotate(dot(x, wk[...])).astype(F32)
    nv_s[...] = dot(x, wv[...]).astype(BF16).astype(F32)

    lh = log2(heads)
    nq = own * 2 * heads
    r0, c0 = iota((nq, heads * group), 0), iota((nq, heads * group), 1)
    source = ((r0 & (heads - 1)) * group) + t * own + (r0 >> (lh + 1))
    order = ones_where(c0 == source).astype(BF16)
    loads["kc"].wait()
    loads["vc"].wait()
    heard(1)
    tell(2)
    arrived(copies)
    q = dot(order, qbuf[...].reshape(heads * group, LANES))
    q = jnp.where((iota((nq, LANES), 1) >> 6) == ((iota((nq, LANES), 0) >> lh) & 1), q, 0.0)
    position = iota((2 * heads, s.length), 1).astype(F32)
    outs = []
    for b in range(own):
        qb = q[b * 2 * heads : (b + 1) * 2 * heads, :]
        score = lax.dot_general(
            qb.astype(BF16), kc[b], (((1,), (1,)), ((), ())), preferred_element_type=F32
        )
        length = jnp.concatenate([len_s[pl.ds(t * own + b, 1), :]] * (s.length // LANES), axis=-1)
        score = jnp.where(position < length, score * 0.125, -jnp.inf)
        own_score = jnp.sum(qb * nk_s[pl.ds(t * own + b, 1), :], axis=-1, keepdims=True) * 0.125
        top = jnp.maximum(jnp.max(score, axis=-1, keepdims=True), own_score)
        e = jnp.exp(score - top)
        e_own = jnp.exp(own_score - top)
        total = jnp.sum(e, axis=-1, keepdims=True) + e_own
        prob = e / total
        prob_own = jnp.broadcast_to(e_own / total, (2 * heads, LANES))
        weight = (prob - lam * pltpu.roll(prob, heads, 0)).astype(BF16)
        weight_own = (prob_own - lam * pltpu.roll(prob_own, heads, 0)).astype(BF16).astype(F32)
        ho = dot(weight, vc[b]) + weight_own * nv_s[pl.ds(t * own + b, 1), :]
        scale = lax.rsqrt(jnp.mean(ho * ho, axis=-1, keepdims=True) + EPS)
        outs.append(ho * scale * hgain[...])
    attbuf[t] = jnp.concatenate(outs, axis=0).astype(BF16)

    copies = gather(2, attbuf.at[t], attbuf)
    heard(2)
    tell(3)
    r0, c0 = iota((heads * group, tp * nq), 0), iota((heads * group, tp * nq), 1)
    lg = log2(group)
    token = r0 & (group - 1)
    source = (token >> lo) * nq + (token & (own - 1)) * (2 * heads) + (r0 >> lg)
    order = ones_where(c0 == source).astype(BF16)
    loads["wo"].wait()
    heard(3)
    tell(4)
    columns = jnp.concatenate([xs[2 * t], xs[2 * t + 1]], axis=-1).astype(F32)
    arrived(copies)
    att = dot(order, attbuf[...].reshape(tp * nq, LANES)).astype(BF16)
    att = jnp.concatenate([att[h * group : (h + 1) * group, :] for h in range(heads)], axis=-1)
    summed = ALPHA * columns + dot(att, wo[...])

    def normed(v, phase, stats, gain):
        mean = jnp.mean(v, axis=-1, keepdims=True)
        center = v - mean
        square = jnp.sum(center * center, axis=-1, keepdims=True)
        stats[t] = jnp.where(lane == 0, mean, jnp.where(lane == 1, square, 0.0))
        copies = gather(phase, stats.at[t], stats)
        if phase == 3:
            heard(4)
            tell(5)
        arrived(copies)
        means = [stats[i][:, 0:1] for i in range(tp)]
        squares = [stats[i][:, 1:2] for i in range(tp)]
        mean = sum(means) / tp
        spread = (sum(squares) + part * sum((m - mean) ** 2 for m in means)) / (tp * part)
        return ((v - mean) * lax.rsqrt(spread + EPS) * gain[:, pl.ds(pl.multiple_of(t * part, part), part)]).astype(BF16)

    settled = normed(summed, 3, stats1, gain1)

    by_expert = (s.experts, cap, LANES)
    there = Exchange(s, ep, dout, xb.at[t], ep_send.at[0], ep_recv.at[0])
    for half in range(2):
        v = dot(place[...], settled[:, half * LANES : (half + 1) * LANES]).astype(BF16)
        dout[half] = v.reshape(by_expert)
    heard(5)
    there.start()

    def x_copy(i, src, dst, to):
        copy = pltpu.make_async_remote_copy(
            src_ref=src,
            dst_ref=dst,
            send_sem=x_send.at[i],
            recv_sem=x_recv.at[i],
            device_id={"tp": to},
            device_id_type=MESH,
        )
        sent.append(copy)
        return copy

    a_next = x_copy(0, xb.at[t, 0], xb.at[t, 0], nxt)
    b_next = x_copy(1, xb.at[t, 1], xb.at[t, 1], nxt)
    a_prev = x_copy(2, xb.at[t, 0], xb.at[t, 0], prv)
    b_prev = x_copy(3, xb.at[t, 1], xb.at[t, 1], prv)
    a_pass = x_copy(4, xb.at[prv, 0], xb.at[prv, 0], nxt)
    b_pass = x_copy(5, xb.at[nxt, 1], xb.at[nxt, 1], prv)
    there.wait_recv()
    a_next.start()
    b_prev.start()
    b_next.start()
    a_prev.start()
    loads["gate"].wait()
    loads["up"].wait()

    def hidden(i):
        x = jnp.concatenate([xb[i, 0].reshape(rows, LANES), xb[i, 1].reshape(rows, LANES)], axis=-1)
        at = pl.ds(pl.multiple_of(i * part, part), part)
        return dot(x, gate[at, :]), dot(x, up[at, :])

    g, u = hidden(t)
    gacc[...] = g
    uacc[...] = u
    a_next.wait_recv()
    a_pass.start()
    b_prev.wait_recv()
    b_pass.start()
    b_next.wait_recv()
    g, u = hidden(prv)
    gacc[...] += g
    uacc[...] += u
    a_prev.wait_recv()
    g, u = hidden(nxt)
    gacc[...] += g
    uacc[...] += u
    loads["down"].wait()
    a_pass.wait_recv()
    b_pass.wait_recv()
    g, u = hidden(far)
    g = jnp.minimum(gacc[...] + g, LIMIT)
    u = jnp.clip(uacc[...] + u, -LIMIT, LIMIT)
    act = (g / (1.0 + jnp.exp(-SLOPE * g)) * (u + 1.0)).astype(BF16)

    def terms(i):
        return dot(act, down[:, pl.ds(pl.multiple_of(i * part, part), part)])

    a_far = x_copy(6, r2o.at[0], r2i.at[0], nxt)
    b_far = x_copy(7, r2o.at[1], r2i.at[1], prv)
    b_near = x_copy(8, rdo.at[0], rdi.at[0], nxt)
    a_near = x_copy(9, rdo.at[1], rdi.at[1], prv)
    a_pair = x_copy(10, rpo.at[0], rpi.at[0], nxt)
    b_pair = x_copy(11, rpo.at[1], rpi.at[1], prv)
    v = terms(far)
    r2o[0] = v[:, :LANES].astype(BF16)
    a_far.start()
    r2o[1] = v[:, LANES:].astype(BF16)
    b_far.start()
    vn = terms(nxt)
    rdo[0] = vn[:, LANES:].astype(BF16)
    b_near.start()
    vp = terms(prv)
    rdo[1] = vp[:, :LANES].astype(BF16)
    a_near.start()
    a_far.wait_recv()
    rpo[0] = (vn[:, :LANES] + r2i[0].astype(F32)).astype(BF16)
    a_pair.start()
    b_far.wait_recv()
    rpo[1] = (vp[:, LANES:] + r2i[1].astype(F32)).astype(BF16)
    b_pair.start()
    v = terms(t)
    back = Exchange(s, ep, eout, einto, ep_send.at[1], ep_recv.at[1])
    a_near.wait_recv()
    a_pair.wait_recv()
    answer = v[:, :LANES] + rpi[0].astype(F32) + rdi[1].astype(F32)
    eout[0] = answer.astype(BF16).reshape(by_expert)
    b_near.wait_recv()
    b_pair.wait_recv()
    answer = v[:, LANES:] + rpi[1].astype(F32) + rdi[0].astype(F32)
    eout[1] = answer.astype(BF16).reshape(by_expert)
    back.start()
    back.wait_recv()

    def combined(half):
        three = dot(pick[...], einto[half].reshape(rows, LANES))
        return three[:group] + three[group : 2 * group] + three[2 * group :]

    routed_a, routed_b = combined(0), combined(1)
    final = ALPHA * settled.astype(F32) + jnp.concatenate([routed_a, routed_b], axis=-1)
    out_ref[...] = normed(final, 4, stats2, gain2)

    for copy in sent:
        copy.wait_send()
    there.wait_send()
    back.wait_send()


def layer(
    nz,
    cap,
    tokens,
    lengths,
    key_cache,
    value_cache,
    query_weight,
    key_weight,
    value_weight,
    lambdas,
    head_gain,
    output_weight,
    norm1_gain,
    routes,
    route_logits,
    gate_weight,
    up_weight,
    down_weight,
    norm2_gain,
):
    tp = lax.axis_size("tp")
    own, width = tokens.shape
    blocks = width // LANES
    group = own * tp
    heads = lambdas.shape[0]
    length = key_cache.shape[1]
    s = Sizes(
        nz, lax.axis_size("ep") // nz, tp, own, blocks, heads, length, routes.shape[1], cap
    )
    rows, part = s.rows, width // tp
    half = key_weight.shape[1] // 4
    freqs = THETA ** (-np.arange(half, dtype=np.float32) / np.float32(half))
    freqs = np.concatenate([freqs] * 4).astype(np.float32).reshape(1, LANES)
    tok = tokens.reshape(own, blocks, LANES).transpose(1, 0, 2).reshape(blocks * own, LANES)
    given = dict(
        lens=lengths.reshape(1, -1),
        freqs=jnp.asarray(freqs),
        routes=routes.T,
        logits=route_logits.T,
        lams=lambdas.reshape(1, -1),
        hgain=head_gain.reshape(1, -1),
        gain1=norm1_gain.reshape(1, -1),
        gain2=norm2_gain.reshape(1, -1),
        wq=query_weight,
        wk=key_weight,
        wv=value_weight,
        kc=key_cache,
        vc=value_cache,
        wo=output_weight,
        gate=gate_weight[0],
        up=up_weight[0],
        down=down_weight[0],
    )
    operands = [given[name] for name in NAMES]

    def b(*shape):
        return pltpu.VMEM(shape, BF16)

    def f(*shape):
        return pltpu.VMEM(shape, F32)

    sem = pltpu.SemaphoreType.DMA
    by_expert = (s.experts, cap, LANES)
    ff = down_weight.shape[1]
    return pl.pallas_call(
        functools.partial(kernel, s),
        out_shape=jax.ShapeDtypeStruct((group, part), BF16),
        in_specs=[pl.BlockSpec(memory_space=pl.ANY)] * (1 + len(operands)),
        out_specs=pl.BlockSpec(memory_space=pltpu.VMEM),
        scratch_shapes=[pltpu.VMEM(a.shape, a.dtype) for a in operands]
        + [
            b(tp, blocks * own, LANES),
            b(blocks, group, LANES),
            b(tp, group, LANES),
            f(group, LANES),
            f(group, LANES),
            f(group, LANES),
            b(tp, own * 2 * heads, LANES),
            f(tp, group, LANES),
            f(tp, group, LANES),
            b(rows, group),
            b(3 * group, rows),
            b(2, *by_expert),
            b(tp, 2, *by_expert),
            f(rows, ff),
            f(rows, ff),
        ]
        + [b(2, rows, LANES)] * 6
        + [b(2, *by_expert)] * 2
        + [
            sem((1 + len(operands),)),
            sem((5, tp - 1)),
            sem((5, tp - 1)),
            sem((12,)),
            sem((12,)),
            sem((2,)),
            sem((2,)),
            pltpu.SemaphoreType.REGULAR((6,)),
        ],
        compiler_params=pltpu.CompilerParams(collective_id=0, has_side_effects=True),
    )(tok, *operands)


def solution(mesh, nz=8, cap=2):
    in_specs = (
        P(("ep", "tp"), None),
        P("ep"),
        P(("ep", "tp"), None, None),
        P(("ep", "tp"), None, None),
        P(None, "tp"),
        P(),
        P(),
        P(),
        P(),
        P(None, "tp"),
        P(),
        P("ep", None),
        P("ep", None),
        P("ep", None, "tp"),
        P("ep", None, "tp"),
        P("ep", "tp", None),
        P(),
    )
    return jax.shard_map(
        functools.partial(layer, nz, cap),
        mesh=mesh,
        in_specs=in_specs,
        out_specs=P("ep", "tp"),
        check_vma=False,
    )
```

```python
import functools

import jax
import jax.numpy as jnp
import numpy as np
from jax import lax
from jax.experimental import pallas as pl
from jax.experimental.pallas import tpu as pltpu
from jax.sharding import PartitionSpec as P

ALPHA = 1.4142135623730951
EPS = 1e-05
THETA = 500000.0
LIMIT = 7.0
SLOPE = 1.702
LANES = 128
SMALL = ("lens", "freqs", "routes", "logits", "lams", "hgain", "gain1", "gain2")
NAMES = SMALL + ("wq", "wk", "wv", "kc", "vc", "wo", "gate", "up", "down")
MESH = pl.DeviceIdType.MESH
BF16 = jnp.bfloat16
F32 = jnp.float32


def log2(n):
    return n.bit_length() - 1


def iota(shape, dim):
    return lax.broadcasted_iota(jnp.int32, shape, dim)


def ones_where(mask):
    return jnp.where(mask, 1.0, 0.0)


def dot(a, b):
    return jnp.dot(a, b, preferred_element_type=F32)


def far_first(n):
    return sorted(range(n), key=lambda d: -min(d, n - d))


class Sizes:
    def __init__(self, nz, nyc, tp, own, blocks, heads, length, topk, cap):
        self.nz, self.nyc, self.tp, self.own = nz, nyc, tp, own
        self.blocks, self.heads, self.length = blocks, heads, length
        self.topk, self.cap = topk, cap
        self.group = own * tp
        self.experts = nz * nyc
        self.rows = nz * nyc * cap


class Exchange:
    def __init__(self, sizes, ep, out, into, send, recv):
        self.sizes, self.ep = sizes, ep
        self.out, self.into, self.send, self.recv = out, into, send, recv

    def start(self, lines):
        planes, tails = lines

        def post(other):
            pltpu.make_async_remote_copy(
                src_ref=self.out.at[:, other],
                dst_ref=self.into.at[:, self.ep],
                send_sem=self.send,
                recv_sem=self.recv,
                device_id={"ep": other},
                device_id_type=MESH,
            ).start()

        for plane in planes:
            for tail in tails:
                if plane is not planes[-1] or tail is not tails[-1]:
                    post(plane + tail)
        for half in range(2):
            self.into[half, self.ep] = self.out[half, self.ep]

    def total(self):
        every = pl.ds(0, self.sizes.experts - 1)
        return pltpu.make_async_remote_copy(
            src_ref=self.out.at[:, every],
            dst_ref=self.into.at[:, every],
            send_sem=self.send,
            recv_sem=self.recv,
            device_id={"ep": lax.rem(self.ep + 1, self.sizes.experts)},
            device_id_type=MESH,
        )

    def wait_recv(self):
        self.total().wait_recv()

    def wait_send(self):
        self.total().wait_send()


def rotation(angle):
    turns = jnp.floor(angle * 0.6366197723675814 + 0.5)
    r = angle - turns * 1.5703125
    r = r - turns * 4.837512969970703125e-4
    r = r - turns * 7.54978995489188216e-8
    q = r * r
    sine = r + r * q * (-1.6666654611e-1 + q * (8.3321608736e-3 - q * 1.9515295891e-4))
    cosine = 4.166664568298827e-2 + q * (-1.388731625493765e-3 + q * 2.443315711809948e-5)
    cosine = 1.0 - 0.5 * q + q * q * cosine
    quarter = turns.astype(jnp.int32)
    odd = (quarter & 1) == 1
    c = jnp.where(odd, sine, cosine)
    n = jnp.where(odd, cosine, sine)
    c = jnp.where(((quarter + 1) & 2) == 2, -c, c)
    n = jnp.where((quarter & 2) == 2, -n, n)
    return c, n


def kernel(
    s,
    *refs,
):
    count = len(NAMES)
    tok_hbm, inputs, out_ref = refs[0], refs[1 : count + 1], refs[count + 1]
    landing, refs = refs[count + 2 : 2 * count + 2], refs[2 * count + 2 :]
    (lens, freqs, routes_t, logits_t, lams, hgain, gain1, gain2) = landing[:8]
    (wq, wk, wv, kc, vc, wo, gate, up, down) = landing[8:]
    (tokbuf, xs, qbuf, nk_s, nv_s, len_s, attbuf, stats1, stats2, place, pick) = refs[:11]
    (dout, xb, gacc, uacc, r2o, r2i, rdo, rdi, rpo, rpi, eout, einto) = refs[11:23]
    (load_sem, tp_send, tp_recv, x_send, x_recv, ep_send, ep_recv, here) = refs[23:]
    ep = lax.axis_index("ep")
    t = lax.axis_index("tp")
    tp, own, group, heads = s.tp, s.own, s.group, s.heads
    rows, cap = s.rows, s.cap
    part = 2 * LANES
    nxt = lax.rem(t + 1, tp)
    far = lax.rem(t + 2, tp)
    prv = lax.rem(t + 3, tp)

    barrier = pltpu.get_barrier_semaphore()
    nz, ny = s.nz, s.nyc // 2
    z, y, c = ep // s.nyc, ep % s.nyc // 2, ep % 2

    def at_z(d):
        return {"ep": lax.rem(z + d + nz, nz) * s.nyc + ep % s.nyc}

    def at_y(d):
        return {"ep": z * s.nyc + lax.rem(y + d + ny, ny) * 2 + c}

    across = {"ep": ep + 1 - 2 * c}

    def pair(at, d, n):
        return [at(e) for e in sorted({d % n, -d % n} - {0})]

    near = pair(at_z, 1, nz) + pair(at_y, 1, ny) + [across]
    near += [{"tp": lax.rem(t + d, tp)} for d in range(1, tp)]
    for device in near:
        pl.semaphore_signal(barrier, inc=1, device_id=device, device_id_type=MESH)

    rounds = [
        pair(at_z, 1, nz),
        pair(at_z, 2, nz),
        pair(at_y, 1, ny),
        pair(at_y, 2, ny),
        pair(at_y, 4, ny),
        [across],
    ]

    def tell(i):
        for device in rounds[i]:
            pl.semaphore_signal(here.at[i], inc=1, device_id=device, device_id_type=MESH)

    def heard(i):
        if rounds[i]:
            pl.semaphore_wait(here.at[i], len(rounds[i]))

    tok_load = pltpu.make_async_copy(tok_hbm, tokbuf.at[t], load_sem.at[len(inputs)])
    tok_load.start()
    loads = {}
    for i, name in enumerate(NAMES):
        loads[name] = pltpu.make_async_copy(inputs[i], landing[i], load_sem.at[i])
        loads[name].start()

    def tp_copies(phase, src, buf):
        return [
            pltpu.make_async_remote_copy(
                src_ref=src,
                dst_ref=buf.at[t],
                send_sem=tp_send.at[phase, d - 1],
                recv_sem=tp_recv.at[phase, d - 1],
                device_id={"tp": lax.rem(t + d, tp)},
                device_id_type=MESH,
            )
            for d in (2, 1, 3)
        ]

    sent = []

    def gather(phase, src, buf):
        copies = tp_copies(phase, src, buf)
        for copy in copies:
            copy.start()
        sent.extend(copies)
        return copies

    def arrived(copies):
        for copy in copies:
            copy.wait_recv()

    tok_load.wait()
    pl.semaphore_wait(barrier, len(near))

    copies = gather(0, tokbuf.at[t], tokbuf)
    tell(0)
    planes = [lax.rem(z + d, nz) * s.nyc for d in far_first(nz)]
    columns = [lax.rem(y + d, ny) * 2 for d in far_first(ny)]
    lines = planes, [column + core for column in columns for core in (1 - c, c)]
    for name in NAMES[:8]:
        loads[name].wait()
    lc = log2(cap)
    logits = logits_t[...]
    raised = jnp.exp(logits - jnp.max(logits, axis=0, keepdims=True))
    left = raised / jnp.sum(raised, axis=0, keepdims=True)
    named = routes_t[...].astype(F32)
    r0, c0 = iota((group, group), 0), iota((group, group), 1)
    upper = ones_where(r0 < c0).astype(BF16)
    lower = ones_where(c0 < r0).astype(BF16)
    same = ones_where(c0 == r0).astype(BF16)

    def upright(v):
        return lax.dot_general(
            same, v.astype(BF16), (((1,), (1,)), ((), ())), preferred_element_type=F32
        )

    routes = upright(named)
    pieces = []
    for i in range(3):
        pieces.append(left.astype(BF16))
        left = left - pieces[-1].astype(F32)
    route_weight = sum(upright(piece) for piece in pieces)
    row = iota((rows, group), 0)
    hits = jnp.zeros((rows, group), F32)
    for k in range(s.topk):
        hits += ones_where(named[k : k + 1, :] == (row >> lc).astype(F32))
    before = dot(hits.astype(BF16), upper)
    place[...] = jnp.where(before == (row & (cap - 1)).astype(F32), hits, 0.0).astype(BF16)
    row = iota((group, rows), 1)
    hits = jnp.zeros((group, rows), F32)
    weighed = jnp.zeros((group, rows), F32)
    for k in range(s.topk):
        hit = routes[:, k : k + 1] == (row >> lc).astype(F32)
        hits += ones_where(hit)
        weighed += jnp.where(hit, route_weight[:, k : k + 1], 0.0)
    before = dot(lower, hits.astype(BF16))
    weighed = jnp.where(before == (row & (cap - 1)).astype(F32), weighed, 0.0)
    for i in range(3):
        piece = weighed.astype(BF16)
        pick[i * group : (i + 1) * group, :] = piece
        weighed = weighed - piece.astype(F32)

    lane = iota((group, LANES), 1)
    lengths = jnp.where(c0 == r0, lens[...].astype(F32), 0.0)
    lengths = jnp.broadcast_to(jnp.sum(lengths, axis=-1, keepdims=True), (group, LANES))
    len_s[...] = lengths
    cosine, sine = rotation(lengths * freqs[...])
    sine = jnp.where((lane & 32) == 0, -sine, sine)
    r0, c0 = iota((2 * heads, heads), 0), iota((2 * heads, heads), 1)
    lam = jnp.where((r0 & (heads - 1)) == c0, lams[...], 0.0)
    lam = jnp.sum(lam, axis=-1, keepdims=True)

    nrow = tp * s.blocks * own
    r0, c0 = iota((nrow, nrow), 0), iota((nrow, nrow), 1)
    lo, lt, lb = log2(own), log2(tp), log2(s.blocks)
    origin = (((r0 >> lo) & (tp - 1)) << (lb + lo)) + ((r0 >> (lo + lt)) << lo) + (r0 & (own - 1))
    order = ones_where(c0 == origin).astype(BF16)
    loads["wq"].wait()
    arrived(copies)
    x = dot(order, tokbuf[...].reshape(nrow, LANES)).astype(BF16)
    xs[...] = x.reshape(s.blocks, group, LANES)
    x = jnp.concatenate([xs[i] for i in range(s.blocks)], axis=-1)

    def rotate(v):
        swapped = jnp.where((lane & 32) == 0, pltpu.roll(v, 96, 1), pltpu.roll(v, 32, 1))
        return (v * cosine + swapped * sine).astype(BF16)

    qbuf[t] = rotate(dot(x, wq[...]))
    copies = gather(1, qbuf.at[t], qbuf)
    heard(0)
    tell(1)
    loads["wk"].wait()
    loads["wv"].wait()
    nk_s[...] = rotate(dot(x, wk[...])).astype(F32)
    nv_s[...] = dot(x, wv[...]).astype(BF16).astype(F32)

    lh = log2(heads)
    nq = own * 2 * heads
    r0, c0 = iota((nq, heads * group), 0), iota((nq, heads * group), 1)
    source = ((r0 & (heads - 1)) * group) + t * own + (r0 >> (lh + 1))
    order = ones_where(c0 == source).astype(BF16)
    loads["kc"].wait()
    loads["vc"].wait()
    heard(1)
    tell(2)
    arrived(copies)
    q = dot(order, qbuf[...].reshape(heads * group, LANES))
    q = jnp.where((iota((nq, LANES), 1) >> 6) == ((iota((nq, LANES), 0) >> lh) & 1), q, 0.0)
    position = iota((2 * heads, s.length), 1).astype(F32)
    outs = []
    for b in range(own):
        qb = q[b * 2 * heads : (b + 1) * 2 * heads, :]
        score = lax.dot_general(
            qb.astype(BF16), kc[b], (((1,), (1,)), ((), ())), preferred_element_type=F32
        )
        length = jnp.concatenate([len_s[pl.ds(t * own + b, 1), :]] * (s.length // LANES), axis=-1)
        score = jnp.where(position < length, score * 0.125, -jnp.inf)
        own_score = jnp.sum(qb * nk_s[pl.ds(t * own + b, 1), :], axis=-1, keepdims=True) * 0.125
        top = jnp.maximum(jnp.max(score, axis=-1, keepdims=True), own_score)
        e = jnp.exp(score - top)
        e_own = jnp.exp(own_score - top)
        total = jnp.sum(e, axis=-1, keepdims=True) + e_own
        prob = e / total
        prob_own = jnp.broadcast_to(e_own / total, (2 * heads, LANES))
        weight = (prob - lam * pltpu.roll(prob, heads, 0)).astype(BF16)
        weight_own = (prob_own - lam * pltpu.roll(prob_own, heads, 0)).astype(BF16).astype(F32)
        ho = dot(weight, vc[b]) + weight_own * nv_s[pl.ds(t * own + b, 1), :]
        scale = lax.rsqrt(jnp.mean(ho * ho, axis=-1, keepdims=True) + EPS)
        outs.append(ho * scale * hgain[...])
    attbuf[t] = jnp.concatenate(outs, axis=0).astype(BF16)

    copies = gather(2, attbuf.at[t], attbuf)
    heard(2)
    tell(3)
    r0, c0 = iota((heads * group, tp * nq), 0), iota((heads * group, tp * nq), 1)
    lg = log2(group)
    token = r0 & (group - 1)
    source = (token >> lo) * nq + (token & (own - 1)) * (2 * heads) + (r0 >> lg)
    order = ones_where(c0 == source).astype(BF16)
    loads["wo"].wait()
    heard(3)
    tell(4)
    columns = jnp.concatenate([xs[2 * t], xs[2 * t + 1]], axis=-1).astype(F32)
    arrived(copies)
    att = dot(order, attbuf[...].reshape(tp * nq, LANES)).astype(BF16)
    att = jnp.concatenate([att[h * group : (h + 1) * group, :] for h in range(heads)], axis=-1)
    summed = ALPHA * columns + dot(att, wo[...])

    def normed(v, phase, stats, gain):
        mean = jnp.mean(v, axis=-1, keepdims=True)
        center = v - mean
        square = jnp.sum(center * center, axis=-1, keepdims=True)
        stats[t] = jnp.where(lane == 0, mean, jnp.where(lane == 1, square, 0.0))
        copies = gather(phase, stats.at[t], stats)
        if phase == 3:
            heard(4)
            tell(5)
        arrived(copies)
        means = [stats[i][:, 0:1] for i in range(tp)]
        squares = [stats[i][:, 1:2] for i in range(tp)]
        mean = sum(means) / tp
        spread = (sum(squares) + part * sum((m - mean) ** 2 for m in means)) / (tp * part)
        return ((v - mean) * lax.rsqrt(spread + EPS) * gain[:, pl.ds(pl.multiple_of(t * part, part), part)]).astype(BF16)

    settled = normed(summed, 3, stats1, gain1)

    by_expert = (s.experts, cap, LANES)
    there = Exchange(s, ep, dout, xb.at[t], ep_send.at[0], ep_recv.at[0])
    for half in range(2):
        v = dot(place[...], settled[:, half * LANES : (half + 1) * LANES]).astype(BF16)
        dout[half] = v.reshape(by_expert)
    heard(5)
    there.start(lines)

    def x_copy(i, src, dst, to):
        copy = pltpu.make_async_remote_copy(
            src_ref=src,
            dst_ref=dst,
            send_sem=x_send.at[i],
            recv_sem=x_recv.at[i],
            device_id={"tp": to},
            device_id_type=MESH,
        )
        sent.append(copy)
        return copy

    a_next = x_copy(0, xb.at[t, 0], xb.at[t, 0], nxt)
    b_next = x_copy(1, xb.at[t, 1], xb.at[t, 1], nxt)
    a_prev = x_copy(2, xb.at[t, 0], xb.at[t, 0], prv)
    b_prev = x_copy(3, xb.at[t, 1], xb.at[t, 1], prv)
    a_pass = x_copy(4, xb.at[prv, 0], xb.at[prv, 0], nxt)
    b_pass = x_copy(5, xb.at[nxt, 1], xb.at[nxt, 1], prv)
    there.wait_recv()
    a_next.start()
    b_prev.start()
    b_next.start()
    a_prev.start()
    loads["gate"].wait()
    loads["up"].wait()

    def hidden(i):
        x = jnp.concatenate([xb[i, 0].reshape(rows, LANES), xb[i, 1].reshape(rows, LANES)], axis=-1)
        at = pl.ds(pl.multiple_of(i * part, part), part)
        return dot(x, gate[at, :]), dot(x, up[at, :])

    g, u = hidden(t)
    gacc[...] = g
    uacc[...] = u
    a_next.wait_recv()
    a_pass.start()
    b_prev.wait_recv()
    b_pass.start()
    b_next.wait_recv()
    g, u = hidden(prv)
    gacc[...] += g
    uacc[...] += u
    a_prev.wait_recv()
    g, u = hidden(nxt)
    gacc[...] += g
    uacc[...] += u
    loads["down"].wait()
    a_pass.wait_recv()
    b_pass.wait_recv()
    g, u = hidden(far)
    g = jnp.minimum(gacc[...] + g, LIMIT)
    u = jnp.clip(uacc[...] + u, -LIMIT, LIMIT)
    act = (g / (1.0 + jnp.exp(-SLOPE * g)) * (u + 1.0)).astype(BF16)

    def terms(i):
        return dot(act, down[:, pl.ds(pl.multiple_of(i * part, part), part)])

    a_far = x_copy(6, r2o.at[0], r2i.at[0], nxt)
    b_far = x_copy(7, r2o.at[1], r2i.at[1], prv)
    b_near = x_copy(8, rdo.at[0], rdi.at[0], nxt)
    a_near = x_copy(9, rdo.at[1], rdi.at[1], prv)
    a_pair = x_copy(10, rpo.at[0], rpi.at[0], nxt)
    b_pair = x_copy(11, rpo.at[1], rpi.at[1], prv)
    v = terms(far)
    r2o[0] = v[:, :LANES].astype(BF16)
    a_far.start()
    r2o[1] = v[:, LANES:].astype(BF16)
    b_far.start()
    vn = terms(nxt)
    rdo[0] = vn[:, LANES:].astype(BF16)
    b_near.start()
    vp = terms(prv)
    rdo[1] = vp[:, :LANES].astype(BF16)
    a_near.start()
    a_far.wait_recv()
    rpo[0] = (vn[:, :LANES] + r2i[0].astype(F32)).astype(BF16)
    a_pair.start()
    b_far.wait_recv()
    rpo[1] = (vp[:, LANES:] + r2i[1].astype(F32)).astype(BF16)
    b_pair.start()
    v = terms(t)
    back = Exchange(s, ep, eout, einto, ep_send.at[1], ep_recv.at[1])
    a_near.wait_recv()
    a_pair.wait_recv()
    answer = v[:, :LANES] + rpi[0].astype(F32) + rdi[1].astype(F32)
    eout[0] = answer.astype(BF16).reshape(by_expert)
    b_near.wait_recv()
    b_pair.wait_recv()
    answer = v[:, LANES:] + rpi[1].astype(F32) + rdi[0].astype(F32)
    eout[1] = answer.astype(BF16).reshape(by_expert)
    back.start(lines)
    back.wait_recv()

    def combined(half):
        three = dot(pick[...], einto[half].reshape(rows, LANES))
        return three[:group] + three[group : 2 * group] + three[2 * group :]

    routed_a, routed_b = combined(0), combined(1)
    final = ALPHA * settled.astype(F32) + jnp.concatenate([routed_a, routed_b], axis=-1)
    out_ref[...] = normed(final, 4, stats2, gain2)

    for copy in sent:
        copy.wait_send()
    there.wait_send()
    back.wait_send()


def layer(
    nz,
    cap,
    tokens,
    lengths,
    key_cache,
    value_cache,
    query_weight,
    key_weight,
    value_weight,
    lambdas,
    head_gain,
    output_weight,
    norm1_gain,
    routes,
    route_logits,
    gate_weight,
    up_weight,
    down_weight,
    norm2_gain,
):
    tp = lax.axis_size("tp")
    own, width = tokens.shape
    blocks = width // LANES
    group = own * tp
    heads = lambdas.shape[0]
    length = key_cache.shape[1]
    s = Sizes(
        nz, lax.axis_size("ep") // nz, tp, own, blocks, heads, length, routes.shape[1], cap
    )
    rows, part = s.rows, width // tp
    half = key_weight.shape[1] // 4
    freqs = THETA ** (-np.arange(half, dtype=np.float32) / np.float32(half))
    freqs = np.concatenate([freqs] * 4).astype(np.float32).reshape(1, LANES)
    tok = tokens.reshape(own, blocks, LANES).transpose(1, 0, 2).reshape(blocks * own, LANES)
    given = dict(
        lens=lengths.reshape(1, -1),
        freqs=jnp.asarray(freqs),
        routes=routes.T,
        logits=route_logits.T,
        lams=lambdas.reshape(1, -1),
        hgain=head_gain.reshape(1, -1),
        gain1=norm1_gain.reshape(1, -1),
        gain2=norm2_gain.reshape(1, -1),
        wq=query_weight,
        wk=key_weight,
        wv=value_weight,
        kc=key_cache,
        vc=value_cache,
        wo=output_weight,
        gate=gate_weight[0],
        up=up_weight[0],
        down=down_weight[0],
    )
    operands = [given[name] for name in NAMES]

    def b(*shape):
        return pltpu.VMEM(shape, BF16)

    def f(*shape):
        return pltpu.VMEM(shape, F32)

    sem = pltpu.SemaphoreType.DMA
    by_expert = (s.experts, cap, LANES)
    ff = down_weight.shape[1]
    return pl.pallas_call(
        functools.partial(kernel, s),
        out_shape=jax.ShapeDtypeStruct((group, part), BF16),
        in_specs=[pl.BlockSpec(memory_space=pl.ANY)] * (1 + len(operands)),
        out_specs=pl.BlockSpec(memory_space=pltpu.VMEM),
        scratch_shapes=[pltpu.VMEM(a.shape, a.dtype) for a in operands]
        + [
            b(tp, blocks * own, LANES),
            b(blocks, group, LANES),
            b(tp, group, LANES),
            f(group, LANES),
            f(group, LANES),
            f(group, LANES),
            b(tp, own * 2 * heads, LANES),
            f(tp, group, LANES),
            f(tp, group, LANES),
            b(rows, group),
            b(3 * group, rows),
            b(2, *by_expert),
            b(tp, 2, *by_expert),
            f(rows, ff),
            f(rows, ff),
        ]
        + [b(2, rows, LANES)] * 6
        + [b(2, *by_expert)] * 2
        + [
            sem((1 + len(operands),)),
            sem((5, tp - 1)),
            sem((5, tp - 1)),
            sem((12,)),
            sem((12,)),
            sem((2,)),
            sem((2,)),
            pltpu.SemaphoreType.REGULAR((6,)),
        ],
        compiler_params=pltpu.CompilerParams(
            collective_id=0, has_side_effects=True
        ),
    )(tok, *operands)


def solution(mesh, nz=8, cap=2):
    in_specs = (
        P(("ep", "tp"), None),
        P("ep"),
        P(("ep", "tp"), None, None),
        P(("ep", "tp"), None, None),
        P(None, "tp"),
        P(),
        P(),
        P(),
        P(),
        P(None, "tp"),
        P(),
        P("ep", None),
        P("ep", None),
        P("ep", None, "tp"),
        P("ep", None, "tp"),
        P("ep", "tp", None),
        P(),
    )
    return jax.shard_map(
        functools.partial(layer, nz, cap),
        mesh=mesh,
        in_specs=in_specs,
        out_specs=P("ep", "tp"),
        check_vma=False,
    )
```

```python
import functools

import jax
import jax.numpy as jnp
import numpy as np
from jax import lax
from jax.experimental import pallas as pl
from jax.experimental.pallas import tpu as pltpu
from jax.sharding import PartitionSpec as P

ALPHA = 1.4142135623730951
EPS = 1e-05
THETA = 500000.0
LIMIT = 7.0
SLOPE = 1.702
LANES = 128
SMALL = ("lens", "freqs", "routes", "logits", "lams", "hgain", "gain1", "gain2")
NAMES = SMALL + ("wq", "wk", "wv", "kc", "vc", "wo", "gate", "up", "down")
MESH = pl.DeviceIdType.MESH
BF16 = jnp.bfloat16
F32 = jnp.float32


def log2(n):
    return n.bit_length() - 1


def iota(shape, dim):
    return lax.broadcasted_iota(jnp.int32, shape, dim)


def ones_where(mask):
    return jnp.where(mask, 1.0, 0.0)


def dot(a, b):
    return jnp.dot(a, b, preferred_element_type=F32)


def far_first(n):
    return sorted(range(n), key=lambda d: -min(d, n - d))


class Sizes:
    def __init__(self, nz, nyc, tp, own, blocks, heads, length, topk, cap):
        self.nz, self.nyc, self.tp, self.own = nz, nyc, tp, own
        self.blocks, self.heads, self.length = blocks, heads, length
        self.topk, self.cap = topk, cap
        self.group = own * tp
        self.experts = nz * nyc
        self.rows = nz * nyc * cap


def post(src, dst, send, recv, device):
    pltpu.make_async_remote_copy(
        src_ref=src,
        dst_ref=dst,
        send_sem=send,
        recv_sem=recv,
        device_id={"ep": device},
        device_id_type=MESH,
    ).start()


def messages(ref, count, send, recv, device):
    some = ref.at[:, pl.ds(0, count)]
    return pltpu.make_async_remote_copy(
        src_ref=some,
        dst_ref=some,
        send_sem=send,
        recv_sem=recv,
        device_id={"ep": device},
        device_id_type=MESH,
    )


def rotation(angle):
    turns = jnp.floor(angle * 0.6366197723675814 + 0.5)
    r = angle - turns * 1.5703125
    r = r - turns * 4.837512969970703125e-4
    r = r - turns * 7.54978995489188216e-8
    q = r * r
    sine = r + r * q * (-1.6666654611e-1 + q * (8.3321608736e-3 - q * 1.9515295891e-4))
    cosine = 4.166664568298827e-2 + q * (-1.388731625493765e-3 + q * 2.443315711809948e-5)
    cosine = 1.0 - 0.5 * q + q * q * cosine
    quarter = turns.astype(jnp.int32)
    odd = (quarter & 1) == 1
    c = jnp.where(odd, sine, cosine)
    n = jnp.where(odd, cosine, sine)
    c = jnp.where(((quarter + 1) & 2) == 2, -c, c)
    n = jnp.where((quarter & 2) == 2, -n, n)
    return c, n


def kernel(
    s,
    *refs,
):
    count = len(NAMES)
    tok_hbm, inputs, out_ref = refs[0], refs[1 : count + 1], refs[count + 1]
    landing, refs = refs[count + 2 : 2 * count + 2], refs[2 * count + 2 :]
    (lens, freqs, routes_t, logits_t, lams, hgain, gain1, gain2) = landing[:8]
    (wq, wk, wv, kc, vc, wo, gate, up, down) = landing[8:]
    (tokbuf, xs, qbuf, nk_s, nv_s, len_s, attbuf, stats1, stats2, place, pick) = refs[:11]
    (dout, xb, r2o, r2i, rdo, rdi, rpo, rpi, eout, einto) = refs[11:21]
    (load_sem, tp_send, tp_recv, x_send, x_recv, ep_send, ep_recv, here) = refs[21:]
    ep = lax.axis_index("ep")
    t = lax.axis_index("tp")
    tp, own, group, heads = s.tp, s.own, s.group, s.heads
    rows, cap = s.rows, s.cap
    part = 2 * LANES
    nxt = lax.rem(t + 1, tp)
    far = lax.rem(t + 2, tp)
    prv = lax.rem(t + 3, tp)

    barrier = pltpu.get_barrier_semaphore()
    nz, ny = s.nz, s.nyc // 2
    z, y, c = ep // s.nyc, ep % s.nyc // 2, ep % 2

    def at_z(d):
        return {"ep": lax.rem(z + d + nz, nz) * s.nyc + ep % s.nyc}

    def at_y(d):
        return {"ep": z * s.nyc + lax.rem(y + d + ny, ny) * 2 + c}

    across = {"ep": ep + 1 - 2 * c}

    def pair(at, d, n):
        return [at(e) for e in sorted({d % n, -d % n} - {0})]

    near = pair(at_z, 1, nz) + pair(at_y, 1, ny) + [across]
    near += [{"tp": lax.rem(t + d, tp)} for d in range(1, tp)]
    for device in near:
        pl.semaphore_signal(barrier, inc=1, device_id=device, device_id_type=MESH)

    rounds = [
        pair(at_z, 1, nz),
        pair(at_z, 2, nz),
        pair(at_y, 1, ny),
        pair(at_y, 2, ny),
        pair(at_y, 4, ny),
        [across],
    ]

    def tell(i):
        for device in rounds[i]:
            pl.semaphore_signal(here.at[i], inc=1, device_id=device, device_id_type=MESH)

    def heard(i):
        if rounds[i]:
            pl.semaphore_wait(here.at[i], len(rounds[i]))

    tok_load = pltpu.make_async_copy(tok_hbm, tokbuf.at[t], load_sem.at[len(inputs)])
    tok_load.start()
    loads = {}
    for i, name in enumerate(NAMES):
        loads[name] = pltpu.make_async_copy(inputs[i], landing[i], load_sem.at[i])

    def tp_copies(phase, src, buf):
        return [
            pltpu.make_async_remote_copy(
                src_ref=src,
                dst_ref=buf.at[t],
                send_sem=tp_send.at[phase, d - 1],
                recv_sem=tp_recv.at[phase, d - 1],
                device_id={"tp": lax.rem(t + d, tp)},
                device_id_type=MESH,
            )
            for d in (2, 1, 3)
        ]

    sent = []

    def gather(phase, src, buf):
        copies = tp_copies(phase, src, buf)
        for copy in copies:
            copy.start()
        sent.extend(copies)
        return copies

    def arrived(copies):
        for copy in copies:
            copy.wait_recv()

    tok_load.wait()
    pl.semaphore_wait(barrier, len(near))

    copies = gather(0, tokbuf.at[t], tokbuf)
    tell(0)
    for load in loads.values():
        load.start()
    planes = [lax.rem(z + d, nz) * s.nyc for d in far_first(nz)]
    origins = [lax.rem(z - d + nz, nz) * s.nyc for d in far_first(nz)]
    columns = [lax.rem(y + d, ny) * 2 for d in far_first(ny)]
    tails = [column + core for column in columns for core in (1 - c, c)]
    line = ep % s.nyc
    for name in NAMES[:8]:
        loads[name].wait()
    lc = log2(cap)
    logits = logits_t[...]
    raised = jnp.exp(logits - jnp.max(logits, axis=0, keepdims=True))
    left = raised / jnp.sum(raised, axis=0, keepdims=True)
    named = routes_t[...].astype(F32)
    r0, c0 = iota((group, group), 0), iota((group, group), 1)
    upper = ones_where(r0 < c0).astype(BF16)
    lower = ones_where(c0 < r0).astype(BF16)
    same = ones_where(c0 == r0).astype(BF16)

    def upright(v):
        return lax.dot_general(
            same, v.astype(BF16), (((1,), (1,)), ((), ())), preferred_element_type=F32
        )

    routes = upright(named)
    pieces = []
    for i in range(3):
        pieces.append(left.astype(BF16))
        left = left - pieces[-1].astype(F32)
    route_weight = sum(upright(piece) for piece in pieces)
    row = iota((rows, group), 0)
    hits = jnp.zeros((rows, group), F32)
    for k in range(s.topk):
        hits += ones_where(named[k : k + 1, :] == (row >> lc).astype(F32))
    before = dot(hits.astype(BF16), upper)
    place[...] = jnp.where(before == (row & (cap - 1)).astype(F32), hits, 0.0).astype(BF16)
    row = iota((group, rows), 1)
    hits = jnp.zeros((group, rows), F32)
    weighed = jnp.zeros((group, rows), F32)
    for k in range(s.topk):
        hit = routes[:, k : k + 1] == (row >> lc).astype(F32)
        hits += ones_where(hit)
        weighed += jnp.where(hit, route_weight[:, k : k + 1], 0.0)
    before = dot(lower, hits.astype(BF16))
    weighed = jnp.where(before == (row & (cap - 1)).astype(F32), weighed, 0.0)
    for i in range(3):
        piece = weighed.astype(BF16)
        pick[i * group : (i + 1) * group, :] = piece
        weighed = weighed - piece.astype(F32)

    lane = iota((group, LANES), 1)
    lengths = jnp.where(c0 == r0, lens[...].astype(F32), 0.0)
    lengths = jnp.broadcast_to(jnp.sum(lengths, axis=-1, keepdims=True), (group, LANES))
    len_s[...] = lengths
    cosine, sine = rotation(lengths * freqs[...])
    sine = jnp.where((lane & 32) == 0, -sine, sine)
    r0, c0 = iota((2 * heads, heads), 0), iota((2 * heads, heads), 1)
    lam = jnp.where((r0 & (heads - 1)) == c0, lams[...], 0.0)
    lam = jnp.sum(lam, axis=-1, keepdims=True)

    nrow = tp * s.blocks * own
    r0, c0 = iota((nrow, nrow), 0), iota((nrow, nrow), 1)
    lo, lt, lb = log2(own), log2(tp), log2(s.blocks)
    origin = (((r0 >> lo) & (tp - 1)) << (lb + lo)) + ((r0 >> (lo + lt)) << lo) + (r0 & (own - 1))
    order = ones_where(c0 == origin).astype(BF16)
    loads["wq"].wait()
    arrived(copies)
    x = dot(order, tokbuf[...].reshape(nrow, LANES)).astype(BF16)
    xs[...] = x.reshape(s.blocks, group, LANES)
    x = jnp.concatenate([xs[i] for i in range(s.blocks)], axis=-1)

    def rotate(v):
        swapped = jnp.where((lane & 32) == 0, pltpu.roll(v, 96, 1), pltpu.roll(v, 32, 1))
        return (v * cosine + swapped * sine).astype(BF16)

    qbuf[t] = rotate(dot(x, wq[...]))
    copies = gather(1, qbuf.at[t], qbuf)
    heard(0)
    tell(1)
    loads["wk"].wait()
    loads["wv"].wait()
    nk_s[...] = rotate(dot(x, wk[...])).astype(F32)
    nv_s[...] = dot(x, wv[...]).astype(BF16).astype(F32)

    lh = log2(heads)
    nq = own * 2 * heads
    r0, c0 = iota((nq, heads * group), 0), iota((nq, heads * group), 1)
    source = ((r0 & (heads - 1)) * group) + t * own + (r0 >> (lh + 1))
    order = ones_where(c0 == source).astype(BF16)
    loads["kc"].wait()
    loads["vc"].wait()
    heard(1)
    tell(2)
    arrived(copies)
    q = dot(order, qbuf[...].reshape(heads * group, LANES))
    q = jnp.where((iota((nq, LANES), 1) >> 6) == ((iota((nq, LANES), 0) >> lh) & 1), q, 0.0)
    position = iota((2 * heads, s.length), 1).astype(F32)
    outs = []
    for b in range(own):
        qb = q[b * 2 * heads : (b + 1) * 2 * heads, :]
        score = lax.dot_general(
            qb.astype(BF16), kc[b], (((1,), (1,)), ((), ())), preferred_element_type=F32
        )
        length = jnp.concatenate([len_s[pl.ds(t * own + b, 1), :]] * (s.length // LANES), axis=-1)
        score = jnp.where(position < length, score * 0.125, -jnp.inf)
        own_score = jnp.sum(qb * nk_s[pl.ds(t * own + b, 1), :], axis=-1, keepdims=True) * 0.125
        top = jnp.maximum(jnp.max(score, axis=-1, keepdims=True), own_score)
        e = jnp.exp(score - top)
        e_own = jnp.exp(own_score - top)
        total = jnp.sum(e, axis=-1, keepdims=True) + e_own
        share = 1.0 / total
        prob = e * share
        prob_own = jnp.broadcast_to(e_own * share, (2 * heads, LANES))
        weight = (prob - lam * pltpu.roll(prob, heads, 0)).astype(BF16)
        weight_own = (prob_own - lam * pltpu.roll(prob_own, heads, 0)).astype(BF16).astype(F32)
        ho = dot(weight, vc[b]) + weight_own * nv_s[pl.ds(t * own + b, 1), :]
        scale = lax.rsqrt(jnp.mean(ho * ho, axis=-1, keepdims=True) + EPS)
        outs.append(ho * scale * hgain[...])
    attbuf[t] = jnp.concatenate(outs, axis=0).astype(BF16)

    copies = gather(2, attbuf.at[t], attbuf)
    heard(2)
    tell(3)
    r0, c0 = iota((heads * group, tp * nq), 0), iota((heads * group, tp * nq), 1)
    lg = log2(group)
    token = r0 & (group - 1)
    source = (token >> lo) * nq + (token & (own - 1)) * (2 * heads) + (r0 >> lg)
    order = ones_where(c0 == source).astype(BF16)
    loads["wo"].wait()
    heard(3)
    tell(4)
    columns = jnp.concatenate([xs[2 * t], xs[2 * t + 1]], axis=-1).astype(F32)
    arrived(copies)
    att = dot(order, attbuf[...].reshape(tp * nq, LANES)).astype(BF16)
    att = jnp.concatenate([att[h * group : (h + 1) * group, :] for h in range(heads)], axis=-1)
    summed = ALPHA * columns + dot(att, wo[...])

    def normed(v, phase, stats, gain):
        mean = jnp.mean(v, axis=-1, keepdims=True)
        center = v - mean
        square = jnp.sum(center * center, axis=-1, keepdims=True)
        stats[t] = jnp.where(lane == 0, mean, jnp.where(lane == 1, square, 0.0))
        copies = gather(phase, stats.at[t], stats)
        if phase == 3:
            heard(4)
            tell(5)
        arrived(copies)
        means = [stats[i][:, 0:1] for i in range(tp)]
        squares = [stats[i][:, 1:2] for i in range(tp)]
        mean = sum(means) / tp
        spread = (sum(squares) + part * sum((m - mean) ** 2 for m in means)) / (tp * part)
        return ((v - mean) * lax.rsqrt(spread + EPS) * gain[:, pl.ds(pl.multiple_of(t * part, part), part)]).astype(BF16)

    settled = normed(summed, 3, stats1, gain1)

    by_expert = (s.experts, cap, LANES)
    mid, last = nz // 2, s.nyc - 1
    for half in range(2):
        v = dot(place[...], settled[:, half * LANES : (half + 1) * LANES]).astype(BF16)
        dout[half] = v.reshape(by_expert)
    heard(5)
    for i in range(nz):
        for j in range(s.nyc):
            if i < nz - 1 or j < last:
                other = planes[i] + tails[j]
                slot = i * s.nyc + line
                post(dout.at[:, other], xb.at[t, :, slot], ep_send.at[0], ep_recv.at[i // mid], other)
    for half in range(2):
        xb[t, half, (nz - 1) * s.nyc + line] = dout[half, ep]

    def x_copy(i, src, dst, to):
        copy = pltpu.make_async_remote_copy(
            src_ref=src,
            dst_ref=dst,
            send_sem=x_send.at[i],
            recv_sem=x_recv.at[i],
            device_id={"tp": to},
            device_id_type=MESH,
        )
        sent.append(copy)
        return copy

    slots = s.experts // 2
    some = rows // 2
    neighbour = across["ep"]
    a_next, b_next, a_prev, b_prev, a_pass, b_pass = [], [], [], [], [], []
    for p in range(2):
        at = pl.ds(p * slots, slots)

        def round_x(i, who, half, to, p=p, at=at):
            return x_copy(12 * p + i, xb.at[who, half, at], xb.at[who, half, at], to)

        a_next.append(round_x(0, t, 0, nxt))
        b_next.append(round_x(1, t, 1, nxt))
        a_prev.append(round_x(2, t, 0, prv))
        b_prev.append(round_x(3, t, 1, prv))
        a_pass.append(round_x(4, prv, 0, nxt))
        b_pass.append(round_x(5, nxt, 1, prv))

    for p in range(2):
        messages(dout, slots - p, ep_send.at[0], ep_recv.at[p], neighbour).wait_recv()
        a_next[p].start()
        b_prev[p].start()
        b_next[p].start()
        a_prev[p].start()
    for p in range(2):
        a_next[p].wait_recv()
        a_pass[p].start()
        b_prev[p].wait_recv()
        b_pass[p].start()
    loads["gate"].wait()
    loads["up"].wait()
    loads["down"].wait()

    def hidden(p):
        at = pl.ds(p * slots, slots)
        g = u = 0.0
        for i in (t, prv, nxt, far):
            x = [xb[i, half, at].reshape(some, LANES) for half in range(2)]
            x = jnp.concatenate(x, axis=-1)
            k = pl.ds(pl.multiple_of(i * part, part), part)
            g = g + dot(x, gate[k, :])
            u = u + dot(x, up[k, :])
        g = jnp.minimum(g, LIMIT)
        u = jnp.clip(u, -LIMIT, LIMIT)
        return (g / (1.0 + jnp.exp(-SLOPE * g)) * (u + 1.0)).astype(BF16)

    def terms(act, i):
        return dot(act, down[:, pl.ds(pl.multiple_of(i * part, part), part)])

    acts, pairs, sums = [], [], []
    for p in range(2):
        b_next[p].wait_recv()
        a_prev[p].wait_recv()
        a_pass[p].wait_recv()
        b_pass[p].wait_recv()
        act = hidden(p)
        acts.append(act)
        hops = [
            x_copy(12 * p + 6, r2o.at[p, 0], r2i.at[p, 0], nxt),
            x_copy(12 * p + 7, r2o.at[p, 1], r2i.at[p, 1], prv),
            x_copy(12 * p + 8, rdo.at[p, 0], rdi.at[p, 0], nxt),
            x_copy(12 * p + 9, rdo.at[p, 1], rdi.at[p, 1], prv),
            x_copy(12 * p + 10, rpo.at[p, 0], rpi.at[p, 0], nxt),
            x_copy(12 * p + 11, rpo.at[p, 1], rpi.at[p, 1], prv),
        ]
        sums.append(hops)
        v = terms(act, far)
        r2o[p, 0] = v[:, :LANES].astype(BF16)
        hops[0].start()
        r2o[p, 1] = v[:, LANES:].astype(BF16)
        hops[1].start()
        vn = terms(act, nxt)
        rdo[p, 0] = vn[:, LANES:].astype(BF16)
        hops[2].start()
        vp = terms(act, prv)
        rdo[p, 1] = vp[:, :LANES].astype(BF16)
        hops[3].start()
        pairs.append((vn[:, :LANES], vp[:, LANES:]))
    for p in range(2):
        hops, (vn, vp) = sums[p], pairs[p]
        hops[0].wait_recv()
        rpo[p, 0] = (vn + r2i[p, 0].astype(F32)).astype(BF16)
        hops[4].start()
        hops[1].wait_recv()
        rpo[p, 1] = (vp + r2i[p, 1].astype(F32)).astype(BF16)
        hops[5].start()
    mine = [terms(act, t) for act in acts]
    for p in range(2):
        hops, v = sums[p], mine[p]
        at = pl.ds(p * slots, slots)
        for i in (2, 3, 4, 5):
            hops[i].wait_recv()
        answer = v[:, :LANES] + rpi[p, 0].astype(F32) + rdi[p, 1].astype(F32)
        eout[0, at] = answer.astype(BF16).reshape(slots, cap, LANES)
        answer = v[:, LANES:] + rpi[p, 1].astype(F32) + rdi[p, 0].astype(F32)
        eout[1, at] = answer.astype(BF16).reshape(slots, cap, LANES)
        for i in range(p * mid, (p + 1) * mid):
            for j in range(s.nyc):
                if i < nz - 1 or j < last:
                    slot = i * s.nyc + tails[j]
                    other = origins[i] + tails[j]
                    post(eout.at[:, slot], einto.at[:, ep], ep_send.at[1], ep_recv.at[2], other)
    for half in range(2):
        einto[half, ep] = eout[half, (nz - 1) * s.nyc + line]
    messages(eout, s.experts - 1, ep_send.at[1], ep_recv.at[2], neighbour).wait_recv()

    def combined(half):
        three = dot(pick[...], einto[half].reshape(rows, LANES))
        return three[:group] + three[group : 2 * group] + three[2 * group :]

    routed_a, routed_b = combined(0), combined(1)
    final = ALPHA * settled.astype(F32) + jnp.concatenate([routed_a, routed_b], axis=-1)
    out_ref[...] = normed(final, 4, stats2, gain2)

    for copy in sent:
        copy.wait_send()
    messages(dout, s.experts - 1, ep_send.at[0], ep_recv.at[0], neighbour).wait_send()
    messages(eout, s.experts - 1, ep_send.at[1], ep_recv.at[2], neighbour).wait_send()


def layer(
    nz,
    cap,
    tokens,
    lengths,
    key_cache,
    value_cache,
    query_weight,
    key_weight,
    value_weight,
    lambdas,
    head_gain,
    output_weight,
    norm1_gain,
    routes,
    route_logits,
    gate_weight,
    up_weight,
    down_weight,
    norm2_gain,
):
    tp = lax.axis_size("tp")
    own, width = tokens.shape
    blocks = width // LANES
    group = own * tp
    heads = lambdas.shape[0]
    length = key_cache.shape[1]
    s = Sizes(
        nz, lax.axis_size("ep") // nz, tp, own, blocks, heads, length, routes.shape[1], cap
    )
    rows, part = s.rows, width // tp
    half = key_weight.shape[1] // 4
    freqs = THETA ** (-np.arange(half, dtype=np.float32) / np.float32(half))
    freqs = np.concatenate([freqs] * 4).astype(np.float32).reshape(1, LANES)
    tok = tokens.reshape(own, blocks, LANES).transpose(1, 0, 2).reshape(blocks * own, LANES)
    given = dict(
        lens=lengths.reshape(1, -1),
        freqs=jnp.asarray(freqs),
        routes=routes.T,
        logits=route_logits.T,
        lams=lambdas.reshape(1, -1),
        hgain=head_gain.reshape(1, -1),
        gain1=norm1_gain.reshape(1, -1),
        gain2=norm2_gain.reshape(1, -1),
        wq=query_weight,
        wk=key_weight,
        wv=value_weight,
        kc=key_cache,
        vc=value_cache,
        wo=output_weight,
        gate=gate_weight[0],
        up=up_weight[0],
        down=down_weight[0],
    )
    operands = [given[name] for name in NAMES]

    def b(*shape):
        return pltpu.VMEM(shape, BF16)

    def f(*shape):
        return pltpu.VMEM(shape, F32)

    sem = pltpu.SemaphoreType.DMA
    by_expert = (s.experts, cap, LANES)
    return pl.pallas_call(
        functools.partial(kernel, s),
        out_shape=jax.ShapeDtypeStruct((group, part), BF16),
        in_specs=[pl.BlockSpec(memory_space=pl.ANY)] * (1 + len(operands)),
        out_specs=pl.BlockSpec(memory_space=pltpu.VMEM),
        scratch_shapes=[pltpu.VMEM(a.shape, a.dtype) for a in operands]
        + [
            b(tp, blocks * own, LANES),
            b(blocks, group, LANES),
            b(tp, group, LANES),
            f(group, LANES),
            f(group, LANES),
            f(group, LANES),
            b(tp, own * 2 * heads, LANES),
            f(tp, group, LANES),
            f(tp, group, LANES),
            b(rows, group),
            b(3 * group, rows),
            b(2, *by_expert),
            b(tp, 2, *by_expert),
        ]
        + [b(2, 2, rows // 2, LANES)] * 6
        + [b(2, *by_expert)] * 2
        + [
            sem((1 + len(operands),)),
            sem((5, tp - 1)),
            sem((5, tp - 1)),
            sem((24,)),
            sem((24,)),
            sem((2,)),
            sem((3,)),
            pltpu.SemaphoreType.REGULAR((6,)),
        ],
        compiler_params=pltpu.CompilerParams(
            collective_id=0, has_side_effects=True
        ),
    )(tok, *operands)


def solution(mesh, nz=8, cap=2):
    in_specs = (
        P(("ep", "tp"), None),
        P("ep"),
        P(("ep", "tp"), None, None),
        P(("ep", "tp"), None, None),
        P(None, "tp"),
        P(),
        P(),
        P(),
        P(),
        P(None, "tp"),
        P(),
        P("ep", None),
        P("ep", None),
        P("ep", None, "tp"),
        P("ep", None, "tp"),
        P("ep", "tp", None),
        P(),
    )
    return jax.shard_map(
        functools.partial(layer, nz, cap),
        mesh=mesh,
        in_specs=in_specs,
        out_specs=P("ep", "tp"),
        check_vma=False,
    )
```

```python
import functools

import jax
import jax.numpy as jnp
import numpy as np
from jax import lax
from jax.experimental import pallas as pl
from jax.experimental.pallas import tpu as pltpu
from jax.sharding import PartitionSpec as P

ALPHA = 1.4142135623730951
EPS = 1e-05
THETA = 500000.0
LIMIT = 7.0
SLOPE = 1.702
LANES = 128
SMALL = ("lens", "freqs", "routes", "logits", "lams", "hgain", "gain1", "gain2")
NAMES = SMALL + ("wq", "wk", "wv", "kc", "vc", "wo", "gate", "up", "down")
MESH = pl.DeviceIdType.MESH
BF16 = jnp.bfloat16
F32 = jnp.float32


def log2(n):
    return n.bit_length() - 1


def iota(shape, dim):
    return lax.broadcasted_iota(jnp.int32, shape, dim)


def ones_where(mask):
    return jnp.where(mask, 1.0, 0.0)


def dot(a, b):
    return jnp.dot(a, b, preferred_element_type=F32)


def far_first(n):
    return sorted(range(n), key=lambda d: -min(d, n - d))


class Sizes:
    def __init__(self, nz, nyc, tp, own, blocks, heads, length, topk, cap):
        self.nz, self.nyc, self.tp, self.own = nz, nyc, tp, own
        self.blocks, self.heads, self.length = blocks, heads, length
        self.topk, self.cap = topk, cap
        self.group = own * tp
        self.experts = nz * nyc
        self.rows = nz * nyc * cap


def post(src, dst, send, recv, device):
    pltpu.make_async_remote_copy(
        src_ref=src,
        dst_ref=dst,
        send_sem=send,
        recv_sem=recv,
        device_id={"ep": device},
        device_id_type=MESH,
    ).start()


def messages(ref, count, send, recv, device):
    some = ref.at[:, pl.ds(0, count)]
    return pltpu.make_async_remote_copy(
        src_ref=some,
        dst_ref=some,
        send_sem=send,
        recv_sem=recv,
        device_id={"ep": device},
        device_id_type=MESH,
    )


def rotation(angle):
    turns = jnp.floor(angle * 0.6366197723675814 + 0.5)
    r = angle - turns * 1.5703125
    r = r - turns * 4.837512969970703125e-4
    r = r - turns * 7.54978995489188216e-8
    q = r * r
    sine = r + r * q * (-1.6666654611e-1 + q * (8.3321608736e-3 - q * 1.9515295891e-4))
    cosine = 4.166664568298827e-2 + q * (-1.388731625493765e-3 + q * 2.443315711809948e-5)
    cosine = 1.0 - 0.5 * q + q * q * cosine
    quarter = turns.astype(jnp.int32)
    odd = (quarter & 1) == 1
    c = jnp.where(odd, sine, cosine)
    n = jnp.where(odd, cosine, sine)
    c = jnp.where(((quarter + 1) & 2) == 2, -c, c)
    n = jnp.where((quarter & 2) == 2, -n, n)
    return c, n


def kernel(
    s,
    *refs,
):
    count = len(NAMES)
    tok_hbm, inputs, out_ref = refs[0], refs[1 : count + 1], refs[count + 1]
    landing, refs = refs[count + 2 : 2 * count + 2], refs[2 * count + 2 :]
    (lens, freqs, routes_t, logits_t, lams, hgain, gain1, gain2) = landing[:8]
    (wq, wk, wv, kc, vc, wo, gate, up, down) = landing[8:]
    (tokbuf, xs, qbuf, nk_s, nv_s, len_s, attbuf, stats1, stats2, place, pick) = refs[:11]
    (dout, xb, rsum_out, rsum_in, eout, einto) = refs[11:17]
    (load_sem, tp_send, tp_recv, x_send, x_recv, ep_send, ep_recv, here) = refs[17:]
    ep = lax.axis_index("ep")
    t = lax.axis_index("tp")
    tp, own, group, heads = s.tp, s.own, s.group, s.heads
    rows, cap = s.rows, s.cap
    part = 2 * LANES
    nxt = lax.rem(t + 1, tp)
    far = lax.rem(t + 2, tp)
    prv = lax.rem(t + 3, tp)

    barrier = pltpu.get_barrier_semaphore()
    nz, ny = s.nz, s.nyc // 2
    z, y, c = ep // s.nyc, ep % s.nyc // 2, ep % 2

    def at_z(d):
        return {"ep": lax.rem(z + d + nz, nz) * s.nyc + ep % s.nyc}

    def at_y(d):
        return {"ep": z * s.nyc + lax.rem(y + d + ny, ny) * 2 + c}

    across = {"ep": ep + 1 - 2 * c}

    def pair(at, d, n):
        return [at(e) for e in sorted({d % n, -d % n} - {0})]

    near = pair(at_z, 1, nz) + pair(at_y, 1, ny) + [across]
    near += [{"tp": lax.rem(t + d, tp)} for d in range(1, tp)]
    for device in near:
        pl.semaphore_signal(barrier, inc=1, device_id=device, device_id_type=MESH)

    rounds = [
        pair(at_z, 1, nz),
        pair(at_z, 2, nz),
        pair(at_y, 1, ny),
        pair(at_y, 2, ny),
        pair(at_y, 4, ny),
        [across],
    ]

    def tell(i):
        for device in rounds[i]:
            pl.semaphore_signal(here.at[i], inc=1, device_id=device, device_id_type=MESH)

    def heard(i):
        if rounds[i]:
            pl.semaphore_wait(here.at[i], len(rounds[i]))

    tok_load = pltpu.make_async_copy(tok_hbm, tokbuf.at[t], load_sem.at[len(inputs)])
    tok_load.start()
    loads = {}
    for i, name in enumerate(NAMES):
        loads[name] = pltpu.make_async_copy(inputs[i], landing[i], load_sem.at[i])

    def tp_copies(phase, src, buf):
        return [
            pltpu.make_async_remote_copy(
                src_ref=src,
                dst_ref=buf.at[t],
                send_sem=tp_send.at[phase, d - 1],
                recv_sem=tp_recv.at[phase, d - 1],
                device_id={"tp": lax.rem(t + d, tp)},
                device_id_type=MESH,
            )
            for d in (2, 1, 3)
        ]

    sent = []

    def gather(phase, src, buf):
        copies = tp_copies(phase, src, buf)
        for copy in copies:
            copy.start()
        sent.extend(copies)
        return copies

    def arrived(copies):
        for copy in copies:
            copy.wait_recv()

    tok_load.wait()
    pl.semaphore_wait(barrier, len(near))

    copies = gather(0, tokbuf.at[t], tokbuf)
    tell(0)
    for load in loads.values():
        load.start()
    planes = [lax.rem(z + d, nz) * s.nyc for d in far_first(nz)]
    origins = [lax.rem(z - d + nz, nz) * s.nyc for d in far_first(nz)]
    columns = [lax.rem(y + d, ny) * 2 for d in far_first(ny)]
    tails = [column + core for column in columns for core in (1 - c, c)]
    line = ep % s.nyc
    for name in NAMES[:8]:
        loads[name].wait()
    lc = log2(cap)
    logits = logits_t[...]
    raised = jnp.exp(logits - jnp.max(logits, axis=0, keepdims=True))
    left = raised / jnp.sum(raised, axis=0, keepdims=True)
    named = routes_t[...].astype(F32)
    r0, c0 = iota((group, group), 0), iota((group, group), 1)
    upper = ones_where(r0 < c0).astype(BF16)
    lower = ones_where(c0 < r0).astype(BF16)
    same = ones_where(c0 == r0).astype(BF16)

    def upright(v):
        return lax.dot_general(
            same, v.astype(BF16), (((1,), (1,)), ((), ())), preferred_element_type=F32
        )

    routes = upright(named)
    pieces = []
    for i in range(3):
        pieces.append(left.astype(BF16))
        left = left - pieces[-1].astype(F32)
    route_weight = sum(upright(piece) for piece in pieces)
    row = iota((rows, group), 0)
    hits = jnp.zeros((rows, group), F32)
    for k in range(s.topk):
        hits += ones_where(named[k : k + 1, :] == (row >> lc).astype(F32))
    before = dot(hits.astype(BF16), upper)
    place[...] = jnp.where(before == (row & (cap - 1)).astype(F32), hits, 0.0).astype(BF16)
    row = iota((group, rows), 1)
    hits = jnp.zeros((group, rows), F32)
    weighed = jnp.zeros((group, rows), F32)
    for k in range(s.topk):
        hit = routes[:, k : k + 1] == (row >> lc).astype(F32)
        hits += ones_where(hit)
        weighed += jnp.where(hit, route_weight[:, k : k + 1], 0.0)
    before = dot(lower, hits.astype(BF16))
    weighed = jnp.where(before == (row & (cap - 1)).astype(F32), weighed, 0.0)
    for i in range(3):
        piece = weighed.astype(BF16)
        pick[i * group : (i + 1) * group, :] = piece
        weighed = weighed - piece.astype(F32)

    lane = iota((group, LANES), 1)
    lengths = jnp.where(c0 == r0, lens[...].astype(F32), 0.0)
    lengths = jnp.broadcast_to(jnp.sum(lengths, axis=-1, keepdims=True), (group, LANES))
    len_s[...] = lengths
    cosine, sine = rotation(lengths * freqs[...])
    sine = jnp.where((lane & 32) == 0, -sine, sine)
    r0, c0 = iota((2 * heads, heads), 0), iota((2 * heads, heads), 1)
    lam = jnp.where((r0 & (heads - 1)) == c0, lams[...], 0.0)
    lam = jnp.sum(lam, axis=-1, keepdims=True)

    nrow = tp * s.blocks * own
    r0, c0 = iota((nrow, nrow), 0), iota((nrow, nrow), 1)
    lo, lt, lb = log2(own), log2(tp), log2(s.blocks)
    origin = (((r0 >> lo) & (tp - 1)) << (lb + lo)) + ((r0 >> (lo + lt)) << lo) + (r0 & (own - 1))
    order = ones_where(c0 == origin).astype(BF16)
    loads["wq"].wait()
    arrived(copies)
    x = dot(order, tokbuf[...].reshape(nrow, LANES)).astype(BF16)
    xs[...] = x.reshape(s.blocks, group, LANES)
    x = jnp.concatenate([xs[i] for i in range(s.blocks)], axis=-1)

    def rotate(v):
        swapped = jnp.where((lane & 32) == 0, pltpu.roll(v, 96, 1), pltpu.roll(v, 32, 1))
        return (v * cosine + swapped * sine).astype(BF16)

    qbuf[t] = rotate(dot(x, wq[...]))
    copies = gather(1, qbuf.at[t], qbuf)
    heard(0)
    tell(1)
    loads["wk"].wait()
    loads["wv"].wait()
    nk_s[...] = rotate(dot(x, wk[...])).astype(F32)
    nv_s[...] = dot(x, wv[...]).astype(BF16).astype(F32)

    lh = log2(heads)
    nq = own * 2 * heads
    r0, c0 = iota((nq, heads * group), 0), iota((nq, heads * group), 1)
    source = ((r0 & (heads - 1)) * group) + t * own + (r0 >> (lh + 1))
    order = ones_where(c0 == source).astype(BF16)
    loads["kc"].wait()
    loads["vc"].wait()
    heard(1)
    tell(2)
    arrived(copies)
    q = dot(order, qbuf[...].reshape(heads * group, LANES))
    q = jnp.where((iota((nq, LANES), 1) >> 6) == ((iota((nq, LANES), 0) >> lh) & 1), q, 0.0)
    position = iota((2 * heads, s.length), 1).astype(F32)
    outs = []
    for b in range(own):
        qb = q[b * 2 * heads : (b + 1) * 2 * heads, :]
        score = lax.dot_general(
            qb.astype(BF16), kc[b], (((1,), (1,)), ((), ())), preferred_element_type=F32
        )
        length = jnp.concatenate([len_s[pl.ds(t * own + b, 1), :]] * (s.length // LANES), axis=-1)
        score = jnp.where(position < length, score * 0.125, -jnp.inf)
        own_score = jnp.sum(qb * nk_s[pl.ds(t * own + b, 1), :], axis=-1, keepdims=True) * 0.125
        top = jnp.maximum(jnp.max(score, axis=-1, keepdims=True), own_score)
        e = jnp.exp(score - top)
        e_own = jnp.exp(own_score - top)
        total = jnp.sum(e, axis=-1, keepdims=True) + e_own
        share = 1.0 / total
        prob = e * share
        prob_own = jnp.broadcast_to(e_own * share, (2 * heads, LANES))
        weight = (prob - lam * pltpu.roll(prob, heads, 0)).astype(BF16)
        weight_own = (prob_own - lam * pltpu.roll(prob_own, heads, 0)).astype(BF16).astype(F32)
        ho = dot(weight, vc[b]) + weight_own * nv_s[pl.ds(t * own + b, 1), :]
        scale = lax.rsqrt(jnp.mean(ho * ho, axis=-1, keepdims=True) + EPS)
        outs.append(ho * scale * hgain[...])
    attbuf[t] = jnp.concatenate(outs, axis=0).astype(BF16)

    copies = gather(2, attbuf.at[t], attbuf)
    heard(2)
    tell(3)
    r0, c0 = iota((heads * group, tp * nq), 0), iota((heads * group, tp * nq), 1)
    lg = log2(group)
    token = r0 & (group - 1)
    source = (token >> lo) * nq + (token & (own - 1)) * (2 * heads) + (r0 >> lg)
    order = ones_where(c0 == source).astype(BF16)
    loads["wo"].wait()
    heard(3)
    tell(4)
    columns = jnp.concatenate([xs[2 * t], xs[2 * t + 1]], axis=-1).astype(F32)
    arrived(copies)
    att = dot(order, attbuf[...].reshape(tp * nq, LANES)).astype(BF16)
    att = jnp.concatenate([att[h * group : (h + 1) * group, :] for h in range(heads)], axis=-1)
    summed = ALPHA * columns + dot(att, wo[...])

    def normed(v, phase, stats, gain):
        mean = jnp.mean(v, axis=-1, keepdims=True)
        center = v - mean
        square = jnp.sum(center * center, axis=-1, keepdims=True)
        stats[t] = jnp.where(lane == 0, mean, jnp.where(lane == 1, square, 0.0))
        copies = gather(phase, stats.at[t], stats)
        if phase == 3:
            heard(4)
            tell(5)
        arrived(copies)
        means = [stats[i][:, 0:1] for i in range(tp)]
        squares = [stats[i][:, 1:2] for i in range(tp)]
        mean = sum(means) / tp
        spread = (sum(squares) + part * sum((m - mean) ** 2 for m in means)) / (tp * part)
        return ((v - mean) * lax.rsqrt(spread + EPS) * gain[:, pl.ds(pl.multiple_of(t * part, part), part)]).astype(BF16)

    settled = normed(summed, 3, stats1, gain1)

    by_expert = (s.experts, cap, LANES)
    mid, last = nz // 2, s.nyc - 1
    for half in range(2):
        v = dot(place[...], settled[:, half * LANES : (half + 1) * LANES]).astype(BF16)
        dout[half] = v.reshape(by_expert)
    heard(5)
    for i in range(nz):
        for j in range(s.nyc):
            if i < nz - 1 or j < last:
                other = planes[i] + tails[j]
                slot = i * s.nyc + line
                post(dout.at[:, other], xb.at[t, :, slot], ep_send.at[0], ep_recv.at[i // mid], other)
    for half in range(2):
        xb[t, half, (nz - 1) * s.nyc + line] = dout[half, ep]

    def x_copy(i, src, dst, to):
        copy = pltpu.make_async_remote_copy(
            src_ref=src,
            dst_ref=dst,
            send_sem=x_send.at[i],
            recv_sem=x_recv.at[i],
            device_id={"tp": to},
            device_id_type=MESH,
        )
        sent.append(copy)
        return copy

    slots = s.experts // 2
    some = rows // 2
    neighbour = across["ep"]
    a_next, b_next, a_prev, b_prev, a_far, b_far = [], [], [], [], [], []
    for p in range(2):
        at = pl.ds(p * slots, slots)

        def round_x(i, who, half, to, p=p, at=at):
            return x_copy(12 * p + i, xb.at[who, half, at], xb.at[who, half, at], to)

        a_next.append(round_x(0, t, 0, nxt))
        b_next.append(round_x(1, t, 1, nxt))
        a_prev.append(round_x(2, t, 0, prv))
        b_prev.append(round_x(3, t, 1, prv))
        a_far.append(round_x(4, t, 0, far))
        b_far.append(round_x(5, t, 1, far))

    for p in range(2):
        messages(dout, slots - p, ep_send.at[0], ep_recv.at[p], neighbour).wait_recv()
        for copy in (a_far, b_far, a_next, b_prev, b_next, a_prev):
            copy[p].start()
    loads["gate"].wait()
    loads["up"].wait()
    loads["down"].wait()

    def hidden(p):
        at = pl.ds(p * slots, slots)
        g = u = 0.0
        for i in (t, prv, nxt, far):
            x = [xb[i, half, at].reshape(some, LANES) for half in range(2)]
            x = jnp.concatenate(x, axis=-1)
            k = pl.ds(pl.multiple_of(i * part, part), part)
            g = g + dot(x, gate[k, :])
            u = u + dot(x, up[k, :])
        g = jnp.minimum(g, LIMIT)
        u = jnp.clip(u, -LIMIT, LIMIT)
        return (g / (1.0 + jnp.exp(-SLOPE * g)) * (u + 1.0)).astype(BF16)

    def terms(act, i):
        return dot(act, down[:, pl.ds(pl.multiple_of(i * part, part), part)])

    acts, sums = [], []
    for p in range(2):
        for copy in (a_next, b_next, a_prev, b_prev, a_far, b_far):
            copy[p].wait_recv()
        act = hidden(p)
        acts.append(act)
        hops = []
        for d, who in ((2, far), (1, nxt), (3, prv)):
            hop = x_copy(12 * p + 5 + d, rsum_out.at[p, d - 1], rsum_in.at[p, d - 1], who)
            rsum_out[p, d - 1] = terms(act, who).astype(BF16)
            hop.start()
            hops.append(hop)
        sums.append(hops)
    mine = [terms(act, t) for act in acts]
    for p in range(2):
        hops, v = sums[p], mine[p]
        at = pl.ds(p * slots, slots)
        for hop in hops:
            hop.wait_recv()
        answer = v + sum(rsum_in[p, d].astype(F32) for d in range(3))
        for half in range(2):
            piece = answer[:, half * LANES : (half + 1) * LANES].astype(BF16)
            eout[half, at] = piece.reshape(slots, cap, LANES)
        for i in range(p * mid, (p + 1) * mid):
            for j in range(s.nyc):
                if i < nz - 1 or j < last:
                    slot = i * s.nyc + tails[j]
                    other = origins[i] + tails[j]
                    post(eout.at[:, slot], einto.at[:, ep], ep_send.at[1], ep_recv.at[2], other)
    for half in range(2):
        einto[half, ep] = eout[half, (nz - 1) * s.nyc + line]
    messages(eout, s.experts - 1, ep_send.at[1], ep_recv.at[2], neighbour).wait_recv()

    def combined(half):
        three = dot(pick[...], einto[half].reshape(rows, LANES))
        return three[:group] + three[group : 2 * group] + three[2 * group :]

    routed_a, routed_b = combined(0), combined(1)
    final = ALPHA * settled.astype(F32) + jnp.concatenate([routed_a, routed_b], axis=-1)
    out_ref[...] = normed(final, 4, stats2, gain2)

    for copy in sent:
        copy.wait_send()
    messages(dout, s.experts - 1, ep_send.at[0], ep_recv.at[0], neighbour).wait_send()
    messages(eout, s.experts - 1, ep_send.at[1], ep_recv.at[2], neighbour).wait_send()


def layer(
    nz,
    cap,
    tokens,
    lengths,
    key_cache,
    value_cache,
    query_weight,
    key_weight,
    value_weight,
    lambdas,
    head_gain,
    output_weight,
    norm1_gain,
    routes,
    route_logits,
    gate_weight,
    up_weight,
    down_weight,
    norm2_gain,
):
    tp = lax.axis_size("tp")
    own, width = tokens.shape
    blocks = width // LANES
    group = own * tp
    heads = lambdas.shape[0]
    length = key_cache.shape[1]
    s = Sizes(
        nz, lax.axis_size("ep") // nz, tp, own, blocks, heads, length, routes.shape[1], cap
    )
    rows, part = s.rows, width // tp
    half = key_weight.shape[1] // 4
    freqs = THETA ** (-np.arange(half, dtype=np.float32) / np.float32(half))
    freqs = np.concatenate([freqs] * 4).astype(np.float32).reshape(1, LANES)
    tok = tokens.reshape(own, blocks, LANES).transpose(1, 0, 2).reshape(blocks * own, LANES)
    given = dict(
        lens=lengths.reshape(1, -1),
        freqs=jnp.asarray(freqs),
        routes=routes.T,
        logits=route_logits.T,
        lams=lambdas.reshape(1, -1),
        hgain=head_gain.reshape(1, -1),
        gain1=norm1_gain.reshape(1, -1),
        gain2=norm2_gain.reshape(1, -1),
        wq=query_weight,
        wk=key_weight,
        wv=value_weight,
        kc=key_cache,
        vc=value_cache,
        wo=output_weight,
        gate=gate_weight[0],
        up=up_weight[0],
        down=down_weight[0],
    )
    operands = [given[name] for name in NAMES]

    def b(*shape):
        return pltpu.VMEM(shape, BF16)

    def f(*shape):
        return pltpu.VMEM(shape, F32)

    sem = pltpu.SemaphoreType.DMA
    by_expert = (s.experts, cap, LANES)
    return pl.pallas_call(
        functools.partial(kernel, s),
        out_shape=jax.ShapeDtypeStruct((group, part), BF16),
        in_specs=[pl.BlockSpec(memory_space=pl.ANY)] * (1 + len(operands)),
        out_specs=pl.BlockSpec(memory_space=pltpu.VMEM),
        scratch_shapes=[pltpu.VMEM(a.shape, a.dtype) for a in operands]
        + [
            b(tp, blocks * own, LANES),
            b(blocks, group, LANES),
            b(tp, group, LANES),
            f(group, LANES),
            f(group, LANES),
            f(group, LANES),
            b(tp, own * 2 * heads, LANES),
            f(tp, group, LANES),
            f(tp, group, LANES),
            b(rows, group),
            b(3 * group, rows),
            b(2, *by_expert),
            b(tp, 2, *by_expert),
        ]
        + [b(2, 3, rows // 2, part)] * 2
        + [b(2, *by_expert)] * 2
        + [
            sem((1 + len(operands),)),
            sem((5, tp - 1)),
            sem((5, tp - 1)),
            sem((24,)),
            sem((24,)),
            sem((2,)),
            sem((3,)),
            pltpu.SemaphoreType.REGULAR((6,)),
        ],
        compiler_params=pltpu.CompilerParams(
            collective_id=0, has_side_effects=True, vmem_limit_bytes=24*2**20
        ),
    )(*[pltpu.with_memory_space_constraint(a, pltpu.HBM) for a in (tok, *operands)])


def solution(mesh, nz=8, cap=2):
    in_specs = (
        P(("ep", "tp"), None),
        P("ep"),
        P(("ep", "tp"), None, None),
        P(("ep", "tp"), None, None),
        P(None, "tp"),
        P(),
        P(),
        P(),
        P(),
        P(None, "tp"),
        P(),
        P("ep", None),
        P("ep", None),
        P("ep", None, "tp"),
        P("ep", None, "tp"),
        P("ep", "tp", None),
        P(),
    )
    return jax.shard_map(
        functools.partial(layer, nz, cap),
        mesh=mesh,
        in_specs=in_specs,
        out_specs=P("ep", "tp"),
        check_vma=False,
    )
```

```python
import functools

import jax
import jax.numpy as jnp
import numpy as np
from jax import lax
from jax.experimental import pallas as pl
from jax.experimental.pallas import tpu as pltpu
from jax.sharding import PartitionSpec as P

ALPHA = 1.4142135623730951
EPS = 1e-05
THETA = 500000.0
LIMIT = 7.0
SLOPE = 1.702
LANES = 128
SMALL = ("lens", "freqs", "routes", "logits", "lams", "hgain", "gain1", "gain2")
NAMES = SMALL + ("wq", "wk", "wv", "kc", "vc", "wo", "gate", "up", "down")
PIECES = 4
MESH = pl.DeviceIdType.MESH
BF16 = jnp.bfloat16
F32 = jnp.float32


def log2(n):
    return n.bit_length() - 1


def iota(shape, dim):
    return lax.broadcasted_iota(jnp.int32, shape, dim)


def ones_where(mask):
    return jnp.where(mask, 1.0, 0.0)


def dot(a, b):
    return jnp.dot(a, b, preferred_element_type=F32)


def far_first(n):
    return sorted(range(n), key=lambda d: -min(d, n - d))


class Sizes:
    def __init__(self, nz, nyc, tp, own, blocks, heads, length, topk, cap):
        self.nz, self.nyc, self.tp, self.own = nz, nyc, tp, own
        self.blocks, self.heads, self.length = blocks, heads, length
        self.topk, self.cap = topk, cap
        self.group = own * tp
        self.experts = nz * nyc
        self.rows = nz * nyc * cap


def post(src, dst, send, recv, device):
    pltpu.make_async_remote_copy(
        src_ref=src,
        dst_ref=dst,
        send_sem=send,
        recv_sem=recv,
        device_id={"ep": device},
        device_id_type=MESH,
    ).start()


def messages(ref, count, send, recv, device):
    some = ref.at[:, pl.ds(0, count)]
    return pltpu.make_async_remote_copy(
        src_ref=some,
        dst_ref=some,
        send_sem=send,
        recv_sem=recv,
        device_id={"ep": device},
        device_id_type=MESH,
    )


def rotation(angle):
    turns = jnp.floor(angle * 0.6366197723675814 + 0.5)
    r = angle - turns * 1.5703125
    r = r - turns * 4.837512969970703125e-4
    r = r - turns * 7.54978995489188216e-8
    q = r * r
    sine = r + r * q * (-1.6666654611e-1 + q * (8.3321608736e-3 - q * 1.9515295891e-4))
    cosine = 4.166664568298827e-2 + q * (-1.388731625493765e-3 + q * 2.443315711809948e-5)
    cosine = 1.0 - 0.5 * q + q * q * cosine
    quarter = turns.astype(jnp.int32)
    odd = (quarter & 1) == 1
    c = jnp.where(odd, sine, cosine)
    n = jnp.where(odd, cosine, sine)
    c = jnp.where(((quarter + 1) & 2) == 2, -c, c)
    n = jnp.where((quarter & 2) == 2, -n, n)
    return c, n


def kernel(
    s,
    *refs,
):
    count = len(NAMES)
    tok_hbm, inputs, out_ref = refs[0], refs[1 : count + 1], refs[count + 1]
    landing, refs = refs[count + 2 : 2 * count + 2], refs[2 * count + 2 :]
    (lens, freqs, routes_t, logits_t, lams, hgain, gain1, gain2) = landing[:8]
    (wq, wk, wv, kc, vc, wo, gate, up, down) = landing[8:]
    (tokbuf, xs, qbuf, nk_s, nv_s, len_s, attbuf, stats1, stats2, place, pick) = refs[:11]
    (dout, xb, rsum_out, rsum_in, eout, einto) = refs[11:17]
    (load_sem, tp_send, tp_recv, x_send, x_recv, ep_send, ep_recv, here) = refs[17:]
    ep = lax.axis_index("ep")
    t = lax.axis_index("tp")
    tp, own, group, heads = s.tp, s.own, s.group, s.heads
    rows, cap = s.rows, s.cap
    part = 2 * LANES
    nxt = lax.rem(t + 1, tp)
    far = lax.rem(t + 2, tp)
    prv = lax.rem(t + 3, tp)

    barrier = pltpu.get_barrier_semaphore()
    nz, ny = s.nz, s.nyc // 2
    z, y, c = ep // s.nyc, ep % s.nyc // 2, ep % 2

    def at_z(d):
        return {"ep": lax.rem(z + d + nz, nz) * s.nyc + ep % s.nyc}

    def at_y(d):
        return {"ep": z * s.nyc + lax.rem(y + d + ny, ny) * 2 + c}

    across = {"ep": ep + 1 - 2 * c}

    def pair(at, d, n):
        return [at(e) for e in sorted({d % n, -d % n} - {0})]

    near = pair(at_z, 1, nz) + pair(at_y, 1, ny) + [across]
    near += [{"tp": lax.rem(t + d, tp)} for d in range(1, tp)]
    for device in near:
        pl.semaphore_signal(barrier, inc=1, device_id=device, device_id_type=MESH)

    rounds = [
        pair(at_z, 1, nz),
        pair(at_z, 2, nz),
        pair(at_y, 1, ny),
        pair(at_y, 2, ny),
        pair(at_y, 4, ny),
        [across],
    ]

    def tell(i):
        for device in rounds[i]:
            pl.semaphore_signal(here.at[i], inc=1, device_id=device, device_id_type=MESH)

    def heard(i):
        if rounds[i]:
            pl.semaphore_wait(here.at[i], len(rounds[i]))

    tok_load = pltpu.make_async_copy(tok_hbm, tokbuf.at[t], load_sem.at[len(inputs)])
    tok_load.start()
    loads = {}
    for i, name in enumerate(NAMES):
        loads[name] = pltpu.make_async_copy(inputs[i], landing[i], load_sem.at[i])

    def tp_copies(phase, src, buf):
        return [
            pltpu.make_async_remote_copy(
                src_ref=src,
                dst_ref=buf.at[t],
                send_sem=tp_send.at[phase, d - 1],
                recv_sem=tp_recv.at[phase, d - 1],
                device_id={"tp": lax.rem(t + d, tp)},
                device_id_type=MESH,
            )
            for d in (2, 1, 3)
        ]

    sent = []

    def gather(phase, src, buf):
        copies = tp_copies(phase, src, buf)
        for copy in copies:
            copy.start()
        sent.extend(copies)
        return copies

    def arrived(copies):
        for copy in copies:
            copy.wait_recv()

    tok_load.wait()
    pl.semaphore_wait(barrier, len(near))

    copies = gather(0, tokbuf.at[t], tokbuf)
    tell(0)
    for load in loads.values():
        load.start()
    planes = [lax.rem(z + d, nz) * s.nyc for d in far_first(nz)]
    origins = [lax.rem(z - d + nz, nz) * s.nyc for d in far_first(nz)]
    columns = [lax.rem(y + d, ny) * 2 for d in far_first(ny)]
    tails = [column + core for column in columns for core in (1 - c, c)]
    line = ep % s.nyc
    for name in NAMES[:8]:
        loads[name].wait()
    lc = log2(cap)
    logits = logits_t[...]
    raised = jnp.exp(logits - jnp.max(logits, axis=0, keepdims=True))
    left = raised / jnp.sum(raised, axis=0, keepdims=True)
    named = routes_t[...].astype(F32)
    r0, c0 = iota((group, group), 0), iota((group, group), 1)
    upper = ones_where(r0 < c0).astype(BF16)
    lower = ones_where(c0 < r0).astype(BF16)
    same = ones_where(c0 == r0).astype(BF16)

    def upright(v):
        return lax.dot_general(
            same, v.astype(BF16), (((1,), (1,)), ((), ())), preferred_element_type=F32
        )

    routes = upright(named)
    pieces = []
    for i in range(3):
        pieces.append(left.astype(BF16))
        left = left - pieces[-1].astype(F32)
    route_weight = sum(upright(piece) for piece in pieces)
    row = iota((rows, group), 0)
    hits = jnp.zeros((rows, group), F32)
    for k in range(s.topk):
        hits += ones_where(named[k : k + 1, :] == (row >> lc).astype(F32))
    before = dot(hits.astype(BF16), upper)
    place[...] = jnp.where(before == (row & (cap - 1)).astype(F32), hits, 0.0).astype(BF16)
    row = iota((group, rows), 1)
    hits = jnp.zeros((group, rows), F32)
    weighed = jnp.zeros((group, rows), F32)
    for k in range(s.topk):
        hit = routes[:, k : k + 1] == (row >> lc).astype(F32)
        hits += ones_where(hit)
        weighed += jnp.where(hit, route_weight[:, k : k + 1], 0.0)
    before = dot(lower, hits.astype(BF16))
    weighed = jnp.where(before == (row & (cap - 1)).astype(F32), weighed, 0.0)
    for i in range(3):
        piece = weighed.astype(BF16)
        pick[i * group : (i + 1) * group, :] = piece
        weighed = weighed - piece.astype(F32)

    lane = iota((group, LANES), 1)
    lengths = jnp.where(c0 == r0, lens[...].astype(F32), 0.0)
    lengths = jnp.broadcast_to(jnp.sum(lengths, axis=-1, keepdims=True), (group, LANES))
    len_s[...] = lengths
    cosine, sine = rotation(lengths * freqs[...])
    sine = jnp.where((lane & 32) == 0, -sine, sine)
    r0, c0 = iota((2 * heads, heads), 0), iota((2 * heads, heads), 1)
    lam = jnp.where((r0 & (heads - 1)) == c0, lams[...], 0.0)
    lam = jnp.sum(lam, axis=-1, keepdims=True)

    nrow = tp * s.blocks * own
    r0, c0 = iota((nrow, nrow), 0), iota((nrow, nrow), 1)
    lo, lt, lb = log2(own), log2(tp), log2(s.blocks)
    origin = (((r0 >> lo) & (tp - 1)) << (lb + lo)) + ((r0 >> (lo + lt)) << lo) + (r0 & (own - 1))
    order = ones_where(c0 == origin).astype(BF16)
    loads["wq"].wait()
    arrived(copies)
    x = dot(order, tokbuf[...].reshape(nrow, LANES)).astype(BF16)
    xs[...] = x.reshape(s.blocks, group, LANES)
    x = jnp.concatenate([xs[i] for i in range(s.blocks)], axis=-1)

    def rotate(v):
        swapped = jnp.where((lane & 32) == 0, pltpu.roll(v, 96, 1), pltpu.roll(v, 32, 1))
        return (v * cosine + swapped * sine).astype(BF16)

    qbuf[t] = rotate(dot(x, wq[...]))
    copies = gather(1, qbuf.at[t], qbuf)
    heard(0)
    tell(1)
    loads["wk"].wait()
    loads["wv"].wait()
    nk_s[...] = rotate(dot(x, wk[...])).astype(F32)
    nv_s[...] = dot(x, wv[...]).astype(BF16).astype(F32)

    lh = log2(heads)
    nq = own * 2 * heads
    r0, c0 = iota((nq, heads * group), 0), iota((nq, heads * group), 1)
    source = ((r0 & (heads - 1)) * group) + t * own + (r0 >> (lh + 1))
    order = ones_where(c0 == source).astype(BF16)
    loads["kc"].wait()
    loads["vc"].wait()
    heard(1)
    tell(2)
    arrived(copies)
    q = dot(order, qbuf[...].reshape(heads * group, LANES))
    q = jnp.where((iota((nq, LANES), 1) >> 6) == ((iota((nq, LANES), 0) >> lh) & 1), q, 0.0)
    position = iota((2 * heads, s.length), 1).astype(F32)
    outs = []
    for b in range(own):
        qb = q[b * 2 * heads : (b + 1) * 2 * heads, :]
        score = lax.dot_general(
            qb.astype(BF16), kc[b], (((1,), (1,)), ((), ())), preferred_element_type=F32
        )
        length = jnp.concatenate([len_s[pl.ds(t * own + b, 1), :]] * (s.length // LANES), axis=-1)
        score = jnp.where(position < length, score * 0.125, -jnp.inf)
        own_score = jnp.sum(qb * nk_s[pl.ds(t * own + b, 1), :], axis=-1, keepdims=True) * 0.125
        top = jnp.maximum(jnp.max(score, axis=-1, keepdims=True), own_score)
        e = jnp.exp(score - top)
        e_own = jnp.exp(own_score - top)
        total = jnp.sum(e, axis=-1, keepdims=True) + e_own
        share = 1.0 / total
        prob = e * share
        prob_own = jnp.broadcast_to(e_own * share, (2 * heads, LANES))
        weight = (prob - lam * pltpu.roll(prob, heads, 0)).astype(BF16)
        weight_own = (prob_own - lam * pltpu.roll(prob_own, heads, 0)).astype(BF16).astype(F32)
        ho = dot(weight, vc[b]) + weight_own * nv_s[pl.ds(t * own + b, 1), :]
        scale = lax.rsqrt(jnp.mean(ho * ho, axis=-1, keepdims=True) + EPS)
        outs.append(ho * scale * hgain[...])
    attbuf[t] = jnp.concatenate(outs, axis=0).astype(BF16)

    copies = gather(2, attbuf.at[t], attbuf)
    heard(2)
    tell(3)
    r0, c0 = iota((heads * group, tp * nq), 0), iota((heads * group, tp * nq), 1)
    lg = log2(group)
    token = r0 & (group - 1)
    source = (token >> lo) * nq + (token & (own - 1)) * (2 * heads) + (r0 >> lg)
    order = ones_where(c0 == source).astype(BF16)
    loads["wo"].wait()
    heard(3)
    tell(4)
    columns = jnp.concatenate([xs[2 * t], xs[2 * t + 1]], axis=-1).astype(F32)
    arrived(copies)
    att = dot(order, attbuf[...].reshape(tp * nq, LANES)).astype(BF16)
    att = jnp.concatenate([att[h * group : (h + 1) * group, :] for h in range(heads)], axis=-1)
    summed = ALPHA * columns + dot(att, wo[...])

    def normed(v, phase, stats, gain):
        mean = jnp.mean(v, axis=-1, keepdims=True)
        center = v - mean
        square = jnp.sum(center * center, axis=-1, keepdims=True)
        stats[t] = jnp.where(lane == 0, mean, jnp.where(lane == 1, square, 0.0))
        copies = gather(phase, stats.at[t], stats)
        if phase == 3:
            heard(4)
            tell(5)
        arrived(copies)
        means = [stats[i][:, 0:1] for i in range(tp)]
        squares = [stats[i][:, 1:2] for i in range(tp)]
        mean = sum(means) / tp
        spread = (sum(squares) + part * sum((m - mean) ** 2 for m in means)) / (tp * part)
        return ((v - mean) * lax.rsqrt(spread + EPS) * gain[:, pl.ds(pl.multiple_of(t * part, part), part)]).astype(BF16)

    settled = normed(summed, 3, stats1, gain1)

    by_expert = (s.experts, cap, LANES)
    mid, last = nz // PIECES, s.nyc - 1
    for half in range(2):
        v = dot(place[...], settled[:, half * LANES : (half + 1) * LANES]).astype(BF16)
        dout[half] = v.reshape(by_expert)
    heard(5)
    for i in range(nz):
        for j in range(s.nyc):
            if i < nz - 1 or j < last:
                other = planes[i] + tails[j]
                slot = i * s.nyc + line
                post(dout.at[:, other], xb.at[t, :, slot], ep_send.at[0], ep_recv.at[i // mid], other)
    for half in range(2):
        xb[t, half, (nz - 1) * s.nyc + line] = dout[half, ep]

    def x_copy(i, src, dst, to):
        copy = pltpu.make_async_remote_copy(
            src_ref=src,
            dst_ref=dst,
            send_sem=x_send.at[i],
            recv_sem=x_recv.at[i],
            device_id={"tp": to},
            device_id_type=MESH,
        )
        sent.append(copy)
        return copy

    slots = s.experts // PIECES
    some = rows // PIECES
    neighbour = across["ep"]
    a_next, b_next, a_prev, b_prev, a_far, b_far = [], [], [], [], [], []
    for p in range(PIECES):
        at = pl.ds(p * slots, slots)

        def round_x(i, who, half, to, p=p, at=at):
            return x_copy(12 * p + i, xb.at[who, half, at], xb.at[who, half, at], to)

        a_next.append(round_x(0, t, 0, nxt))
        b_next.append(round_x(1, t, 1, nxt))
        a_prev.append(round_x(2, t, 0, prv))
        b_prev.append(round_x(3, t, 1, prv))
        a_far.append(round_x(4, t, 0, far))
        b_far.append(round_x(5, t, 1, far))

    for p in range(PIECES):
        messages(dout, slots - (p == PIECES - 1), ep_send.at[0], ep_recv.at[p], neighbour).wait_recv()
        for copy in (a_far, b_far, a_next, b_prev, b_next, a_prev):
            copy[p].start()
    loads["gate"].wait()
    loads["up"].wait()
    loads["down"].wait()

    def hidden(p):
        at = pl.ds(p * slots, slots)
        g = u = 0.0
        for i in (t, prv, nxt, far):
            x = [xb[i, half, at].reshape(some, LANES) for half in range(2)]
            x = jnp.concatenate(x, axis=-1)
            k = pl.ds(pl.multiple_of(i * part, part), part)
            g = g + dot(x, gate[k, :])
            u = u + dot(x, up[k, :])
        g = jnp.minimum(g, LIMIT)
        u = jnp.clip(u, -LIMIT, LIMIT)
        return (g / (1.0 + jnp.exp(-SLOPE * g)) * (u + 1.0)).astype(BF16)

    def terms(act, i):
        return dot(act, down[:, pl.ds(pl.multiple_of(i * part, part), part)])

    acts, sums = [], []
    for p in range(PIECES):
        for copy in (a_next, b_next, a_prev, b_prev, a_far, b_far):
            copy[p].wait_recv()
        act = hidden(p)
        acts.append(act)
        hops = []
        for d, who in ((2, far), (1, nxt), (3, prv)):
            hop = x_copy(12 * p + 5 + d, rsum_out.at[p, d - 1], rsum_in.at[p, d - 1], who)
            rsum_out[p, d - 1] = terms(act, who).astype(BF16)
            hop.start()
            hops.append(hop)
        sums.append(hops)
    mine = [terms(act, t) for act in acts]
    for p in range(PIECES):
        hops, v = sums[p], mine[p]
        at = pl.ds(p * slots, slots)
        for hop in hops:
            hop.wait_recv()
        answer = v + sum(rsum_in[p, d].astype(F32) for d in range(3))
        for half in range(2):
            piece = answer[:, half * LANES : (half + 1) * LANES].astype(BF16)
            eout[half, at] = piece.reshape(slots, cap, LANES)
        for i in range(p * mid, (p + 1) * mid):
            for j in range(s.nyc):
                if i < nz - 1 or j < last:
                    slot = i * s.nyc + tails[j]
                    other = origins[i] + tails[j]
                    post(eout.at[:, slot], einto.at[:, ep], ep_send.at[1], ep_recv.at[PIECES], other)
    for half in range(2):
        einto[half, ep] = eout[half, (nz - 1) * s.nyc + line]
    messages(eout, s.experts - 1, ep_send.at[1], ep_recv.at[PIECES], neighbour).wait_recv()

    def combined(half):
        three = dot(pick[...], einto[half].reshape(rows, LANES))
        return three[:group] + three[group : 2 * group] + three[2 * group :]

    routed_a, routed_b = combined(0), combined(1)
    final = ALPHA * settled.astype(F32) + jnp.concatenate([routed_a, routed_b], axis=-1)
    out_ref[...] = normed(final, 4, stats2, gain2)

    for copy in sent:
        copy.wait_send()
    messages(dout, s.experts - 1, ep_send.at[0], ep_recv.at[0], neighbour).wait_send()
    messages(eout, s.experts - 1, ep_send.at[1], ep_recv.at[PIECES], neighbour).wait_send()


def layer(
    nz,
    cap,
    tokens,
    lengths,
    key_cache,
    value_cache,
    query_weight,
    key_weight,
    value_weight,
    lambdas,
    head_gain,
    output_weight,
    norm1_gain,
    routes,
    route_logits,
    gate_weight,
    up_weight,
    down_weight,
    norm2_gain,
):
    tp = lax.axis_size("tp")
    own, width = tokens.shape
    blocks = width // LANES
    group = own * tp
    heads = lambdas.shape[0]
    length = key_cache.shape[1]
    s = Sizes(
        nz, lax.axis_size("ep") // nz, tp, own, blocks, heads, length, routes.shape[1], cap
    )
    rows, part = s.rows, width // tp
    half = key_weight.shape[1] // 4
    freqs = THETA ** (-np.arange(half, dtype=np.float32) / np.float32(half))
    freqs = np.concatenate([freqs] * 4).astype(np.float32).reshape(1, LANES)
    tok = tokens.reshape(own, blocks, LANES).transpose(1, 0, 2).reshape(blocks * own, LANES)
    given = dict(
        lens=lengths.reshape(1, -1),
        freqs=jnp.asarray(freqs),
        routes=routes.T,
        logits=route_logits.T,
        lams=lambdas.reshape(1, -1),
        hgain=head_gain.reshape(1, -1),
        gain1=norm1_gain.reshape(1, -1),
        gain2=norm2_gain.reshape(1, -1),
        wq=query_weight,
        wk=key_weight,
        wv=value_weight,
        kc=key_cache,
        vc=value_cache,
        wo=output_weight,
        gate=gate_weight[0],
        up=up_weight[0],
        down=down_weight[0],
    )
    operands = [given[name] for name in NAMES]

    def b(*shape):
        return pltpu.VMEM(shape, BF16)

    def f(*shape):
        return pltpu.VMEM(shape, F32)

    sem = pltpu.SemaphoreType.DMA
    by_expert = (s.experts, cap, LANES)
    return pl.pallas_call(
        functools.partial(kernel, s),
        out_shape=jax.ShapeDtypeStruct((group, part), BF16),
        in_specs=[pl.BlockSpec(memory_space=pl.ANY)] * (1 + len(operands)),
        out_specs=pl.BlockSpec(memory_space=pltpu.VMEM),
        scratch_shapes=[pltpu.VMEM(a.shape, a.dtype) for a in operands]
        + [
            b(tp, blocks * own, LANES),
            b(blocks, group, LANES),
            b(tp, group, LANES),
            f(group, LANES),
            f(group, LANES),
            f(group, LANES),
            b(tp, own * 2 * heads, LANES),
            f(tp, group, LANES),
            f(tp, group, LANES),
            b(rows, group),
            b(3 * group, rows),
            b(2, *by_expert),
            b(tp, 2, *by_expert),
        ]
        + [b(PIECES, 3, rows // PIECES, part)] * 2
        + [b(2, *by_expert)] * 2
        + [
            sem((1 + len(operands),)),
            sem((5, tp - 1)),
            sem((5, tp - 1)),
            sem((12 * PIECES,)),
            sem((12 * PIECES,)),
            sem((2,)),
            sem((PIECES + 1,)),
            pltpu.SemaphoreType.REGULAR((6,)),
        ],
        compiler_params=pltpu.CompilerParams(
            collective_id=0, has_side_effects=True, vmem_limit_bytes=24*2**20
        ),
    )(*[pltpu.with_memory_space_constraint(a, pltpu.HBM) for a in (tok, *operands)])


def solution(mesh, nz=8, cap=2):
    in_specs = (
        P(("ep", "tp"), None),
        P("ep"),
        P(("ep", "tp"), None, None),
        P(("ep", "tp"), None, None),
        P(None, "tp"),
        P(),
        P(),
        P(),
        P(),
        P(None, "tp"),
        P(),
        P("ep", None),
        P("ep", None),
        P("ep", None, "tp"),
        P("ep", None, "tp"),
        P("ep", "tp", None),
        P(),
    )
    return jax.shard_map(
        functools.partial(layer, nz, cap),
        mesh=mesh,
        in_specs=in_specs,
        out_specs=P("ep", "tp"),
        check_vma=False,
    )
```

```python
import functools

import jax
import jax.numpy as jnp
import numpy as np
from jax import lax
from jax.experimental import pallas as pl
from jax.experimental.pallas import tpu as pltpu
from jax.sharding import PartitionSpec as P

ALPHA = 1.4142135623730951
EPS = 1e-05
THETA = 500000.0
LIMIT = 7.0
SLOPE = 1.702
LANES = 128
SMALL = ("lens", "freqs", "routes", "logits", "lams", "hgain", "gain1", "gain2")
NAMES = SMALL + ("wq", "wk", "wv", "kc", "vc", "wo", "gate", "up", "down")
PIECES = 4
MESH = pl.DeviceIdType.MESH
BF16 = jnp.bfloat16
F32 = jnp.float32


def log2(n):
    return n.bit_length() - 1


def iota(shape, dim):
    return lax.broadcasted_iota(jnp.int32, shape, dim)


def ones_where(mask):
    return jnp.where(mask, 1.0, 0.0)


def dot(a, b):
    return jnp.dot(a, b, preferred_element_type=F32)


def far_first(n):
    return sorted(range(n), key=lambda d: -min(d, n - d))


class Sizes:
    def __init__(self, nz, nyc, tp, own, blocks, heads, length, topk, cap):
        self.nz, self.nyc, self.tp, self.own = nz, nyc, tp, own
        self.blocks, self.heads, self.length = blocks, heads, length
        self.topk, self.cap = topk, cap
        self.group = own * tp
        self.experts = nz * nyc
        self.rows = nz * nyc * cap


def post(src, dst, send, recv, device):
    pltpu.make_async_remote_copy(
        src_ref=src,
        dst_ref=dst,
        send_sem=send,
        recv_sem=recv,
        device_id={"ep": device},
        device_id_type=MESH,
    ).start()


def messages(ref, count, send, recv, device):
    some = ref.at[:, pl.ds(0, count)]
    return pltpu.make_async_remote_copy(
        src_ref=some,
        dst_ref=some,
        send_sem=send,
        recv_sem=recv,
        device_id={"ep": device},
        device_id_type=MESH,
    )


def rotation(angle):
    turns = jnp.floor(angle * 0.6366197723675814 + 0.5)
    r = angle - turns * 1.5703125
    r = r - turns * 4.837512969970703125e-4
    r = r - turns * 7.54978995489188216e-8
    q = r * r
    sine = r + r * q * (-1.6666654611e-1 + q * (8.3321608736e-3 - q * 1.9515295891e-4))
    cosine = 4.166664568298827e-2 + q * (-1.388731625493765e-3 + q * 2.443315711809948e-5)
    cosine = 1.0 - 0.5 * q + q * q * cosine
    quarter = turns.astype(jnp.int32)
    odd = (quarter & 1) == 1
    c = jnp.where(odd, sine, cosine)
    n = jnp.where(odd, cosine, sine)
    c = jnp.where(((quarter + 1) & 2) == 2, -c, c)
    n = jnp.where((quarter & 2) == 2, -n, n)
    return c, n


def kernel(
    s,
    *refs,
):
    count = len(NAMES)
    tok_hbm, inputs, out_ref = refs[0], refs[1 : count + 1], refs[count + 1]
    landing, refs = refs[count + 2 : 2 * count + 2], refs[2 * count + 2 :]
    (lens, freqs, routes_t, logits_t, lams, hgain, gain1, gain2) = landing[:8]
    (wq, wk, wv, kc, vc, wo, gate, up, down) = landing[8:]
    (tokbuf, xs, qbuf, nk_s, nv_s, len_s, attbuf, stats1, stats2, place, pick) = refs[:11]
    (dout, xb, rsum_out, rsum_in, eout, einto) = refs[11:17]
    (load_sem, tp_send, tp_recv, x_send, x_recv, ep_send, ep_recv, here) = refs[17:]
    ep = lax.axis_index("ep")
    t = lax.axis_index("tp")
    tp, own, group, heads = s.tp, s.own, s.group, s.heads
    rows, cap = s.rows, s.cap
    part = 2 * LANES
    nxt = lax.rem(t + 1, tp)
    far = lax.rem(t + 2, tp)
    prv = lax.rem(t + 3, tp)

    barrier = pltpu.get_barrier_semaphore()
    nz, ny = s.nz, s.nyc // 2
    z, y, c = ep // s.nyc, ep % s.nyc // 2, ep % 2

    def at_z(d):
        return {"ep": lax.rem(z + d + nz, nz) * s.nyc + ep % s.nyc}

    def at_y(d):
        return {"ep": z * s.nyc + lax.rem(y + d + ny, ny) * 2 + c}

    across = {"ep": ep + 1 - 2 * c}

    def pair(at, d, n):
        return [at(e) for e in sorted({d % n, -d % n} - {0})]

    near = pair(at_z, 1, nz) + pair(at_y, 1, ny) + [across]
    near += [{"tp": lax.rem(t + d, tp)} for d in range(1, tp)]
    for device in near:
        pl.semaphore_signal(barrier, inc=1, device_id=device, device_id_type=MESH)

    rounds = [
        pair(at_z, 1, nz),
        pair(at_z, 2, nz),
        pair(at_y, 1, ny),
        pair(at_y, 2, ny),
        pair(at_y, 4, ny),
        [across],
    ]

    def tell(i):
        for device in rounds[i]:
            pl.semaphore_signal(here.at[i], inc=1, device_id=device, device_id_type=MESH)

    def heard(i):
        if rounds[i]:
            pl.semaphore_wait(here.at[i], len(rounds[i]))

    tok_load = pltpu.make_async_copy(tok_hbm, tokbuf.at[t], load_sem.at[len(inputs)])
    tok_load.start()
    loads = {}
    for i, name in enumerate(NAMES):
        loads[name] = pltpu.make_async_copy(inputs[i], landing[i], load_sem.at[i])

    def tp_copies(phase, src, buf):
        return [
            pltpu.make_async_remote_copy(
                src_ref=src,
                dst_ref=buf.at[t],
                send_sem=tp_send.at[phase, d - 1],
                recv_sem=tp_recv.at[phase, d - 1],
                device_id={"tp": lax.rem(t + d, tp)},
                device_id_type=MESH,
            )
            for d in (2, 1, 3)
        ]

    sent = []

    def gather(phase, src, buf):
        copies = tp_copies(phase, src, buf)
        for copy in copies:
            copy.start()
        sent.extend(copies)
        return copies

    def arrived(copies):
        for copy in copies:
            copy.wait_recv()

    tok_load.wait()
    pl.semaphore_wait(barrier, len(near))

    copies = gather(0, tokbuf.at[t], tokbuf)
    tell(0)
    for load in loads.values():
        load.start()
    planes = [lax.rem(z + d, nz) * s.nyc for d in far_first(nz)]
    origins = [lax.rem(z - d + nz, nz) * s.nyc for d in far_first(nz)]
    columns = [lax.rem(y + d, ny) * 2 for d in far_first(ny)]
    tails = [column + core for column in columns for core in (1 - c, c)]
    line = ep % s.nyc
    for name in NAMES[:8]:
        loads[name].wait()
    lc = log2(cap)
    logits = logits_t[...]
    raised = jnp.exp(logits - jnp.max(logits, axis=0, keepdims=True))
    left = raised / jnp.sum(raised, axis=0, keepdims=True)
    named = routes_t[...].astype(F32)
    r0, c0 = iota((group, group), 0), iota((group, group), 1)
    upper = ones_where(r0 < c0).astype(BF16)
    lower = ones_where(c0 < r0).astype(BF16)
    same = ones_where(c0 == r0).astype(BF16)

    def upright(v):
        return lax.dot_general(
            same, v.astype(BF16), (((1,), (1,)), ((), ())), preferred_element_type=F32
        )

    routes = upright(named)
    pieces = []
    for i in range(3):
        pieces.append(left.astype(BF16))
        left = left - pieces[-1].astype(F32)
    route_weight = sum(upright(piece) for piece in pieces)
    row = iota((rows, group), 0)
    hits = jnp.zeros((rows, group), F32)
    for k in range(s.topk):
        hits += ones_where(named[k : k + 1, :] == (row >> lc).astype(F32))
    before = dot(hits.astype(BF16), upper)
    place[...] = jnp.where(before == (row & (cap - 1)).astype(F32), hits, 0.0).astype(BF16)
    row = iota((group, rows), 1)
    hits = jnp.zeros((group, rows), F32)
    weighed = jnp.zeros((group, rows), F32)
    for k in range(s.topk):
        hit = routes[:, k : k + 1] == (row >> lc).astype(F32)
        hits += ones_where(hit)
        weighed += jnp.where(hit, route_weight[:, k : k + 1], 0.0)
    before = dot(lower, hits.astype(BF16))
    weighed = jnp.where(before == (row & (cap - 1)).astype(F32), weighed, 0.0)
    for i in range(3):
        piece = weighed.astype(BF16)
        pick[i * group : (i + 1) * group, :] = piece
        weighed = weighed - piece.astype(F32)

    lane = iota((group, LANES), 1)
    lengths = jnp.where(c0 == r0, lens[...].astype(F32), 0.0)
    lengths = jnp.broadcast_to(jnp.sum(lengths, axis=-1, keepdims=True), (group, LANES))
    len_s[...] = lengths
    cosine, sine = rotation(lengths * freqs[...])
    sine = jnp.where((lane & 32) == 0, -sine, sine)
    r0, c0 = iota((2 * heads, heads), 0), iota((2 * heads, heads), 1)
    lam = jnp.where((r0 & (heads - 1)) == c0, lams[...], 0.0)
    lam = jnp.sum(lam, axis=-1, keepdims=True)

    nrow = tp * s.blocks * own
    r0, c0 = iota((nrow, nrow), 0), iota((nrow, nrow), 1)
    lo, lt, lb = log2(own), log2(tp), log2(s.blocks)
    origin = (((r0 >> lo) & (tp - 1)) << (lb + lo)) + ((r0 >> (lo + lt)) << lo) + (r0 & (own - 1))
    order = ones_where(c0 == origin).astype(BF16)
    loads["wq"].wait()
    arrived(copies)
    x = dot(order, tokbuf[...].reshape(nrow, LANES)).astype(BF16)
    xs[...] = x.reshape(s.blocks, group, LANES)
    x = jnp.concatenate([xs[i] for i in range(s.blocks)], axis=-1)

    def rotate(v):
        swapped = jnp.where((lane & 32) == 0, pltpu.roll(v, 96, 1), pltpu.roll(v, 32, 1))
        return (v * cosine + swapped * sine).astype(BF16)

    qbuf[t] = rotate(dot(x, wq[...]))
    copies = gather(1, qbuf.at[t], qbuf)
    heard(0)
    tell(1)
    loads["wk"].wait()
    loads["wv"].wait()
    nk_s[...] = rotate(dot(x, wk[...])).astype(F32)
    nv_s[...] = dot(x, wv[...]).astype(BF16).astype(F32)

    lh = log2(heads)
    nq = own * 2 * heads
    r0, c0 = iota((nq, heads * group), 0), iota((nq, heads * group), 1)
    source = ((r0 & (heads - 1)) * group) + t * own + (r0 >> (lh + 1))
    order = ones_where(c0 == source).astype(BF16)
    loads["kc"].wait()
    loads["vc"].wait()
    heard(1)
    tell(2)
    arrived(copies)
    q = dot(order, qbuf[...].reshape(heads * group, LANES))
    q = jnp.where((iota((nq, LANES), 1) >> 6) == ((iota((nq, LANES), 0) >> lh) & 1), q, 0.0)
    position = iota((2 * heads, s.length), 1).astype(F32)
    outs = []
    for b in range(own):
        qb = q[b * 2 * heads : (b + 1) * 2 * heads, :]
        score = lax.dot_general(
            qb.astype(BF16), kc[b], (((1,), (1,)), ((), ())), preferred_element_type=F32
        )
        length = jnp.concatenate([len_s[pl.ds(t * own + b, 1), :]] * (s.length // LANES), axis=-1)
        score = jnp.where(position < length, score * 0.125, -jnp.inf)
        own_score = jnp.sum(qb * nk_s[pl.ds(t * own + b, 1), :], axis=-1, keepdims=True) * 0.125
        top = jnp.maximum(jnp.max(score, axis=-1, keepdims=True), own_score)
        e = jnp.exp(score - top)
        e_own = jnp.exp(own_score - top)
        total = jnp.sum(e, axis=-1, keepdims=True) + e_own
        share = 1.0 / total
        prob = e * share
        prob_own = jnp.broadcast_to(e_own * share, (2 * heads, LANES))
        weight = (prob - lam * pltpu.roll(prob, heads, 0)).astype(BF16)
        weight_own = (prob_own - lam * pltpu.roll(prob_own, heads, 0)).astype(BF16).astype(F32)
        ho = dot(weight, vc[b]) + weight_own * nv_s[pl.ds(t * own + b, 1), :]
        scale = lax.rsqrt(jnp.mean(ho * ho, axis=-1, keepdims=True) + EPS)
        outs.append(ho * scale * hgain[...])
    attbuf[t] = jnp.concatenate(outs, axis=0).astype(BF16)

    copies = gather(2, attbuf.at[t], attbuf)
    heard(2)
    tell(3)
    r0, c0 = iota((heads * group, tp * nq), 0), iota((heads * group, tp * nq), 1)
    lg = log2(group)
    token = r0 & (group - 1)
    source = (token >> lo) * nq + (token & (own - 1)) * (2 * heads) + (r0 >> lg)
    order = ones_where(c0 == source).astype(BF16)
    loads["wo"].wait()
    heard(3)
    tell(4)
    columns = jnp.concatenate([xs[2 * t], xs[2 * t + 1]], axis=-1).astype(F32)
    arrived(copies)
    att = dot(order, attbuf[...].reshape(tp * nq, LANES)).astype(BF16)
    att = jnp.concatenate([att[h * group : (h + 1) * group, :] for h in range(heads)], axis=-1)
    summed = ALPHA * columns + dot(att, wo[...])

    def normed(v, phase, stats, gain):
        mean = jnp.mean(v, axis=-1, keepdims=True)
        center = v - mean
        square = jnp.sum(center * center, axis=-1, keepdims=True)
        stats[t] = jnp.where(lane == 0, mean, jnp.where(lane == 1, square, 0.0))
        copies = gather(phase, stats.at[t], stats)
        if phase == 3:
            heard(4)
            tell(5)
        arrived(copies)
        means = [stats[i][:, 0:1] for i in range(tp)]
        squares = [stats[i][:, 1:2] for i in range(tp)]
        mean = sum(means) / tp
        spread = (sum(squares) + part * sum((m - mean) ** 2 for m in means)) / (tp * part)
        return ((v - mean) * lax.rsqrt(spread + EPS) * gain[:, pl.ds(pl.multiple_of(t * part, part), part)]).astype(BF16)

    settled = normed(summed, 3, stats1, gain1)

    by_expert = (s.experts, cap, LANES)
    mid, last = nz // PIECES, s.nyc - 1
    for half in range(2):
        v = dot(place[...], settled[:, half * LANES : (half + 1) * LANES]).astype(BF16)
        dout[half] = v.reshape(by_expert)
    heard(5)
    for i in range(nz):
        for j in range(s.nyc):
            if i < nz - 1 or j < last:
                other = planes[i] + tails[j]
                slot = i * s.nyc + line
                post(dout.at[:, other], xb.at[t, :, slot], ep_send.at[0], ep_recv.at[i // mid], other)
    for half in range(2):
        xb[t, half, (nz - 1) * s.nyc + line] = dout[half, ep]

    def x_copy(i, src, dst, to):
        copy = pltpu.make_async_remote_copy(
            src_ref=src,
            dst_ref=dst,
            send_sem=x_send.at[i],
            recv_sem=x_recv.at[i],
            device_id={"tp": to},
            device_id_type=MESH,
        )
        sent.append(copy)
        return copy

    slots = s.experts // PIECES
    some = rows // PIECES
    neighbour = across["ep"]
    gathers = []
    for p in range(PIECES):
        block = xb.at[t, :, pl.ds(p * slots, slots)]
        gathers.append([x_copy(6 * p + i, block, block, to) for i, to in enumerate((far, nxt, prv))])
        messages(dout, slots - (p == PIECES - 1), ep_send.at[0], ep_recv.at[p], neighbour).wait_recv()
        for copy in gathers[p]:
            copy.start()
    loads["gate"].wait()
    loads["up"].wait()
    loads["down"].wait()

    def hidden(p):
        at = pl.ds(p * slots, slots)
        g = u = 0.0
        for i in (t, prv, nxt, far):
            x = [xb[i, half, at].reshape(some, LANES) for half in range(2)]
            x = jnp.concatenate(x, axis=-1)
            k = pl.ds(pl.multiple_of(i * part, part), part)
            g = g + dot(x, gate[k, :])
            u = u + dot(x, up[k, :])
        g = jnp.minimum(g, LIMIT)
        u = jnp.clip(u, -LIMIT, LIMIT)
        return (g / (1.0 + jnp.exp(-SLOPE * g)) * (u + 1.0)).astype(BF16)

    def terms(act, i):
        return dot(act, down[:, pl.ds(pl.multiple_of(i * part, part), part)])

    acts, sums = [], []
    for p in range(PIECES):
        for copy in gathers[p]:
            copy.wait_recv()
        act = hidden(p)
        acts.append(act)
        hops = []
        for d, who in ((2, far), (1, nxt), (3, prv)):
            hop = x_copy(6 * p + 2 + d, rsum_out.at[p, d - 1], rsum_in.at[p, d - 1], who)
            rsum_out[p, d - 1] = terms(act, who).astype(BF16)
            hop.start()
            hops.append(hop)
        sums.append(hops)
    mine = [terms(act, t) for act in acts]
    for p in range(PIECES):
        hops, v = sums[p], mine[p]
        at = pl.ds(p * slots, slots)
        for hop in hops:
            hop.wait_recv()
        answer = v + sum(rsum_in[p, d].astype(F32) for d in range(3))
        for half in range(2):
            piece = answer[:, half * LANES : (half + 1) * LANES].astype(BF16)
            eout[half, at] = piece.reshape(slots, cap, LANES)
        for i in range(p * mid, (p + 1) * mid):
            for j in range(s.nyc):
                if i < nz - 1 or j < last:
                    slot = i * s.nyc + tails[j]
                    other = origins[i] + tails[j]
                    post(eout.at[:, slot], einto.at[:, ep], ep_send.at[1], ep_recv.at[PIECES], other)
    for half in range(2):
        einto[half, ep] = eout[half, (nz - 1) * s.nyc + line]
    messages(eout, s.experts - 1, ep_send.at[1], ep_recv.at[PIECES], neighbour).wait_recv()

    def combined(half):
        three = dot(pick[...], einto[half].reshape(rows, LANES))
        return three[:group] + three[group : 2 * group] + three[2 * group :]

    routed_a, routed_b = combined(0), combined(1)
    final = ALPHA * settled.astype(F32) + jnp.concatenate([routed_a, routed_b], axis=-1)
    out_ref[...] = normed(final, 4, stats2, gain2)

    for copy in sent:
        copy.wait_send()
    messages(dout, s.experts - 1, ep_send.at[0], ep_recv.at[0], neighbour).wait_send()
    messages(eout, s.experts - 1, ep_send.at[1], ep_recv.at[PIECES], neighbour).wait_send()


def layer(
    nz,
    cap,
    tokens,
    lengths,
    key_cache,
    value_cache,
    query_weight,
    key_weight,
    value_weight,
    lambdas,
    head_gain,
    output_weight,
    norm1_gain,
    routes,
    route_logits,
    gate_weight,
    up_weight,
    down_weight,
    norm2_gain,
):
    tp = lax.axis_size("tp")
    own, width = tokens.shape
    blocks = width // LANES
    group = own * tp
    heads = lambdas.shape[0]
    length = key_cache.shape[1]
    s = Sizes(
        nz, lax.axis_size("ep") // nz, tp, own, blocks, heads, length, routes.shape[1], cap
    )
    rows, part = s.rows, width // tp
    half = key_weight.shape[1] // 4
    freqs = THETA ** (-np.arange(half, dtype=np.float32) / np.float32(half))
    freqs = np.concatenate([freqs] * 4).astype(np.float32).reshape(1, LANES)
    tok = tokens.reshape(own, blocks, LANES).transpose(1, 0, 2).reshape(blocks * own, LANES)
    given = dict(
        lens=lengths.reshape(1, -1),
        freqs=jnp.asarray(freqs),
        routes=routes.T,
        logits=route_logits.T,
        lams=lambdas.reshape(1, -1),
        hgain=head_gain.reshape(1, -1),
        gain1=norm1_gain.reshape(1, -1),
        gain2=norm2_gain.reshape(1, -1),
        wq=query_weight,
        wk=key_weight,
        wv=value_weight,
        kc=key_cache,
        vc=value_cache,
        wo=output_weight,
        gate=gate_weight[0],
        up=up_weight[0],
        down=down_weight[0],
    )
    operands = [given[name] for name in NAMES]

    def b(*shape):
        return pltpu.VMEM(shape, BF16)

    def f(*shape):
        return pltpu.VMEM(shape, F32)

    sem = pltpu.SemaphoreType.DMA
    by_expert = (s.experts, cap, LANES)
    return pl.pallas_call(
        functools.partial(kernel, s),
        out_shape=jax.ShapeDtypeStruct((group, part), BF16),
        in_specs=[pl.BlockSpec(memory_space=pl.ANY)] * (1 + len(operands)),
        out_specs=pl.BlockSpec(memory_space=pltpu.VMEM),
        scratch_shapes=[pltpu.VMEM(a.shape, a.dtype) for a in operands]
        + [
            b(tp, blocks * own, LANES),
            b(blocks, group, LANES),
            b(tp, group, LANES),
            f(group, LANES),
            f(group, LANES),
            f(group, LANES),
            b(tp, own * 2 * heads, LANES),
            f(tp, group, LANES),
            f(tp, group, LANES),
            b(rows, group),
            b(3 * group, rows),
            b(2, *by_expert),
            b(tp, 2, *by_expert),
        ]
        + [b(PIECES, 3, rows // PIECES, part)] * 2
        + [b(2, *by_expert)] * 2
        + [
            sem((1 + len(operands),)),
            sem((5, tp - 1)),
            sem((5, tp - 1)),
            sem((6 * PIECES,)),
            sem((6 * PIECES,)),
            sem((2,)),
            sem((PIECES + 1,)),
            pltpu.SemaphoreType.REGULAR((6,)),
        ],
        compiler_params=pltpu.CompilerParams(
            collective_id=0, has_side_effects=True, vmem_limit_bytes=24*2**20
        ),
    )(*[pltpu.with_memory_space_constraint(a, pltpu.HBM) for a in (tok, *operands)])


def solution(mesh, nz=8, cap=2):
    in_specs = (
        P(("ep", "tp"), None),
        P("ep"),
        P(("ep", "tp"), None, None),
        P(("ep", "tp"), None, None),
        P(None, "tp"),
        P(),
        P(),
        P(),
        P(),
        P(None, "tp"),
        P(),
        P("ep", None),
        P("ep", None),
        P("ep", None, "tp"),
        P("ep", None, "tp"),
        P("ep", "tp", None),
        P(),
    )
    return jax.shard_map(
        functools.partial(layer, nz, cap),
        mesh=mesh,
        in_specs=in_specs,
        out_specs=P("ep", "tp"),
        check_vma=False,
    )
```
